256 devices in a mesh: fs: 32 (over z, x), tp: 8 (over y, core).
Axes of the slice: x: 4, y: 4, z: 8, core: 2. Of those that a mesh axis runs over, the one named last changes fastest.
Arguments:
- tokens: bfloat16 [32768, 2048], P(('fs', 'tp')), may hold values from -6 to 6
- gate_pre: bfloat16 [32768, 5632], P('fs', 'tp'), may hold values from -6 to 6
- value_pre: bfloat16 [32768, 5632], P('fs', 'tp'), may hold values from -6 to 6
- up_gate_w: bfloat16 [2048, 5632], P('fs', 'tp'), may hold values from -0.078125 to 0.078125
- up_value_w: bfloat16 [2048, 5632], P('fs', 'tp'), may hold values from -0.078125 to 0.078125
- conv_weight: float32 [3, 5632], P(None, 'tp'), may hold values from -3 to 3
- conv_bias: float32 [5632], P('tp'), may hold values from -3 to 3
- hidden_grad: bfloat16 [32768, 5632], P('fs', 'tp'), may hold values from -6 to 6
Outputs:
- input_grad: bfloat16 [32768, 2048], P(('fs', 'tp'))
- up_gate_grad: float32 [2048, 5632], P('fs', 'tp')
- up_value_grad: float32 [2048, 5632], P('fs', 'tp')
- conv_weight_grad: float32 [3, 5632], P(None, 'tp')
- conv_bias_grad: float32 [5632], P('tp')
The draws below stay inside these ranges and needn't reach their ends.
All inputs are finite; a program needn't handle non-finite values.
Results may differ from the reference program's by a relative error of at most 0.013.
Values may be sent and summed in bfloat16 or wider, within the bound.
A program may use at most 128 MiB of HBM per device.

```python
import jax
import jax.numpy as jnp
from jax import lax

D = 2048
FF = 5632
ROWS = 1024
TOKENS = 32768
N_FS = 32
N_TP = 8


def with_spikes(result, rng, source, target, shards_of, factor):
    owner, partner = [(jnp.arange(result.shape[dim]) // (result.shape[dim] // shards_of)).reshape([-1 if axis == dim else 1 for axis in range(result.ndim)]) for dim in (source, target)]
    chosen = jax.random.permutation(rng, shards_of)[partner]
    strong = (owner == chosen) | (owner == (partner + shards_of // 2) % shards_of)
    return jnp.where(strong, factor * result, result)


def block_scale(stream_key, shape, cuts, low, largest):
    def one(dim, blocks):
        draws = jax.random.uniform(jax.random.fold_in(jax.random.fold_in(stream_key, 6), dim), (blocks,), jnp.float32, low / len(cuts), largest / len(cuts))
        return jnp.repeat(jnp.exp(draws), shape[dim] // blocks).reshape((-1,) + (1,) * (len(shape) - dim - 1))

    loudness = one(*cuts[0])
    for cut in cuts[1:]:
        loudness = loudness * one(*cut)
    return loudness


def scatter_about(stream_key, dims, spread, limit, shards=(), kind=jnp.bfloat16):
    entries = spread * jax.random.normal(stream_key, dims, jnp.float32)
    if shards:
        entries = entries * block_scale(stream_key, dims, shards, -0.22, 0.18)
    return jnp.clip(entries, -limit, limit).astype(kind)


def heavy_noise(stream_key, dims, deviation, reach, shards, heavy, dtype=jnp.bfloat16):
    result = deviation * jax.random.normal(stream_key, dims, jnp.float32)
    if shards:
        result = result * block_scale(stream_key, dims, shards, -0.22, 0.18)
    return jnp.clip(with_spikes(result, jax.random.fold_in(stream_key, 3), *heavy), -reach, reach).astype(dtype)


def setup_inputs(seed: int = 0) -> dict:
    splits = jax.random.split(jax.random.key(seed), 9)
    tokens = scatter_about(splits[0], (TOKENS, D), 1.0, 6.0, ((0, 256),))
    gate_pre = scatter_about(splits[1], (TOKENS, FF), 1.0, 6.0, ((0, 32), (1, 8)))
    value_pre = scatter_about(splits[2], (TOKENS, FF), 1.0, 6.0, ((0, 32), (1, 8)))
    up_gate_w = scatter_about(splits[3], (D, FF), FF ** -0.5, 0.078125, ((0, 32), (1, 8)))
    up_value_w = scatter_about(splits[4], (D, FF), FF ** -0.5, 0.078125, ((0, 32), (1, 8)))
    conv_weight = scatter_about(splits[5], (3, FF), 0.6, 3.0, ((1, 8),), jnp.float32)
    conv_bias = scatter_about(splits[6], (FF,), 0.5, 3.0, ((0, 8),), jnp.float32)
    hidden_grad = heavy_noise(splits[7], (TOKENS, FF), 1.0, 6.0, ((0, 32), (1, 8)), (0, 1, 32, 2.75))
    return dict(tokens=tokens, gate_pre=gate_pre, value_pre=value_pre, up_gate_w=up_gate_w, up_value_w=up_value_w, conv_weight=conv_weight, conv_bias=conv_bias, hidden_grad=hidden_grad)


def conv_forward(pre_gate, conv_weight, conv_bias):
    length = pre_gate.shape[0]
    padded = jnp.pad(pre_gate, ((2, 0), (0, 0)))
    return conv_bias + conv_weight[0] * padded[:length] + conv_weight[1] * padded[1:length + 1] + conv_weight[2] * padded[2:]

def reference(tokens, gate_pre, value_pre, up_gate_w, up_value_w, conv_weight, conv_bias, hidden_grad):
    col_count = FF // N_TP
    scale = float(TOKENS) ** (-0.5)

    def one_seq(carry, items):
        tok_rows, gate_rows, value_rows, grad_rows = items
        gate_float = gate_rows.astype(jnp.float32)
        gate_conv = conv_forward(gate_float, conv_weight, conv_bias)
        active, gelu_back = jax.vjp(jax.nn.gelu, gate_conv)
        grad_float = grad_rows.astype(jnp.float32)
        value_grad = (grad_float * active).astype(jnp.bfloat16)
        conv_grad = gelu_back(grad_float * value_rows.astype(jnp.float32))[0]
        shifted = jnp.pad(conv_grad, ((0, 2), (0, 0)))
        gate_grad = (conv_weight[2] * conv_grad + conv_weight[1] * shifted[1:ROWS + 1] + conv_weight[0] * shifted[2:]).astype(jnp.bfloat16)
        padded = jnp.pad(gate_float, ((2, 0), (0, 0)))
        conv_terms = jnp.stack([lax.optimization_barrier(jnp.sum(conv_grad * padded[:ROWS], axis=0)), lax.optimization_barrier(jnp.sum(conv_grad * padded[1:ROWS + 1], axis=0)), lax.optimization_barrier(jnp.sum(conv_grad * padded[2:], axis=0)), lax.optimization_barrier(jnp.sum(conv_grad, axis=0))])
        gate_term = jnp.dot(tok_rows.T, gate_grad, preferred_element_type=jnp.float32)
        value_term = jnp.dot(tok_rows.T, value_grad, preferred_element_type=jnp.float32)
        parts = jnp.einsum('rkc,dkc->krd', gate_grad.reshape(ROWS, N_TP, col_count).astype(jnp.float32), up_gate_w.reshape(D, N_TP, col_count).astype(jnp.float32))
        parts = parts + jnp.einsum('rkc,dkc->krd', value_grad.reshape(ROWS, N_TP, col_count).astype(jnp.float32), up_value_w.reshape(D, N_TP, col_count).astype(jnp.float32))
        rounded = lax.optimization_barrier(parts.astype(jnp.bfloat16))
        input_rows = lax.optimization_barrier(jnp.sum(rounded.astype(jnp.float32), axis=0)).astype(jnp.bfloat16)
        return ((carry[0] + gate_term, carry[1] + value_term, carry[2] + conv_terms), input_rows)
    init = (jnp.zeros((D, FF), jnp.float32), jnp.zeros((D, FF), jnp.float32), jnp.zeros((4, FF), jnp.float32))
    items = (tokens.reshape(N_FS, ROWS, D), gate_pre.reshape(N_FS, ROWS, FF), value_pre.reshape(N_FS, ROWS, FF), hidden_grad.reshape(N_FS, ROWS, FF))
    totals, input_seqs = lax.scan(one_seq, init, items)
    input_grad = input_seqs.reshape(TOKENS, D)
    conv_total = totals[2] * scale
    return (input_grad, totals[0] * scale, totals[1] * scale, conv_total[:3], conv_total[3])
```

```python
import functools

import jax
import jax.numpy as jnp
from jax import lax
from jax.experimental import pallas as pl
from jax.experimental.pallas import tpu as pltpu
from jax.sharding import PartitionSpec as P

MESH = pl.DeviceIdType.MESH
F32 = jnp.float32
BF16 = jnp.bfloat16
NC = 2
SUB = 64
LANES = 128

LINK = 46_650.0
TWIN = 300_000.0
HOP = 2.2
TWIN_HOP = 1.0


class Plan:
    def __init__(self):
        self.messages = {}
        self.tasks = {}

    def message(self, name, link, source, target, device, nbytes):
        self.messages[name] = (link, source, target, device, nbytes)

    def task(self, name, rank, cost, body=None, waits=(), after=(), sends=()):
        self.tasks[name] = (rank, cost, body, tuple(waits), tuple(after), tuple(sends))

    def order(self):
        arrival, free, ended, listed = {}, {}, {}, []
        left = dict(self.tasks)
        now = 0.0
        while left:
            best = None
            for name, (rank, cost, body, waits, after, sends) in left.items():
                if any(w not in arrival for w in waits) or any(a not in ended for a in after):
                    continue
                ready = max([now] + [arrival[w] for w in waits])
                key = (ready > now, ready if ready > now else 0.0, rank)
                if best is None or key < best[0]:
                    best = (key, name, ready)
            name, ready = best[1], best[2]
            rank, cost, body, waits, after, sends = left.pop(name)
            now = ready + cost
            ended[name] = now
            listed.append(name)
            for m in sends:
                link, nbytes = self.messages[m][0], self.messages[m][4]
                start = max(now, free.get(link, 0.0))
                rate, hop = (TWIN, TWIN_HOP) if link == "twin" else (LINK, HOP)
                free[link] = start + nbytes / rate
                arrival[m] = free[link] + hop
        self.length = now
        self.ended = ended
        return listed


def nbytes_of(ref):
    size = ref.dtype.itemsize
    for s in ref.shape:
        size *= s
    return size


def kernel(
    dims,
    tokens,
    gate_in,
    value_in,
    wg_in,
    wv_in,
    cw_in,
    cb_in,
    hidden_in,
    ig_out,
    gg_out,
    vg_out,
    cwg_out,
    cbg_out,
    gate,
    value,
    hidden,
    wgs,
    wvs,
    cw,
    cb,
    tok,
    wa,
    wb,
    ga,
    gb,
    pa,
    pb,
    az_up,
    az_dn,
    ax_up,
    ax_dn,
    bx_up,
    bx_dn,
    bz_up,
    bz_dn,
    igp,
    twin_in,
    y_up,
    y_dn,
    later,
    terms,
    cx,
    cz,
    load_sem,
    send_sem,
    recv_sem,
):
    nz, nx, ny = dims
    fs, tp = lax.axis_index("fs"), lax.axis_index("tp")
    z, x, y, c = fs // nx, fs % nx, tp // NC, tp % NC
    rows, width = gate.shape
    mine = tok.shape[0] // (ny * NC)
    whole = width // LANES * LANES
    rest = width - whole
    shard = wgs.shape[0]
    group = nx * shard
    scale = float(rows * nz * nx) ** (-0.5)

    def at_z(d):
        return (((z + d + nz) % nz) * nx + x, tp)

    def at_x(d):
        return (z * nx + (x + d + nx) % nx, tp)

    def at_y(d):
        return (fs, ((y + d + ny) % ny) * NC + c)

    twin = (fs, y * NC + 1 - c)

    loads = {}
    for i, (name, source, target) in enumerate(
        (
            ("wg", wg_in, wgs),
            ("wv", wv_in, wvs),
            ("tok", tokens, tok.at[pl.ds(tp * mine, mine)]),
            ("gate", gate_in, gate),
            ("value", value_in, value),
            ("hidden", hidden_in, hidden),
            ("cw", cw_in, cw),
            ("cb", cb_in, cb),
        )
    ):
        loads[name] = pltpu.make_async_copy(source, target, load_sem.at[i])
        loads[name].start()
    barrier = pltpu.get_barrier_semaphore()
    peers = (at_z(1), at_z(-1), at_x(1), at_x(-1), at_y(1), at_y(-1), twin)
    for peer in peers:
        pl.semaphore_signal(barrier, inc=1, device_id=peer, device_id_type=MESH)

    loads["wg"].wait()
    loads["wv"].wait()
    wa[fs] = wgs[:, :whole]
    wb[fs, :, :whole] = wvs[:, :whole]
    wb[fs, :, whole:] = jnp.concatenate(
        [wvs[:, whole:].astype(F32), wgs[:, whole:].astype(F32)], axis=1
    ).astype(BF16)
    later[...] = jnp.zeros_like(later)
    terms[...] = jnp.zeros_like(terms)
    pl.semaphore_wait(barrier, len(peers))

    plan = Plan()

    def ring_at(axis):
        return {
            "z": (nz, z, at_z),
            "x": (nx, x, at_x),
            "y": (ny, y, at_y),
        }[axis]

    def gather(name, axis, block, half, rank, extra=None, first=None):
        n, me, to = ring_at(axis)
        far = n // 2

        def idx(d):
            return (me + d + n) % n

        for h in range(1, far + 1):
            up, dn = idx(1 - h), idx(h - 1)
            su, sd = (block(up), block(dn)) if h < far else (half(up, 0), half(dn, 1))
            plan.message(f"{name}.up{h}", axis + "+", su, su, to(1), nbytes_of(su))
            plan.message(f"{name}.dn{h}", axis + "-", sd, sd, to(-1), nbytes_of(sd))
        ends = {0: first}
        for h in range(1, far):
            for way, sign in (("up", -1), ("dn", 1)):
                task = f"{name}.{way}{h}"
                plan.task(
                    task,
                    rank,
                    0.05,
                    waits=[task],
                    sends=[f"{name}.{way}{h + 1}"] + (extra(sign * h) if extra else []),
                )
                ends[sign * h] = task
        plan.task(
            f"{name}.last",
            rank,
            0.05,
            waits=[f"{name}.up{far}", f"{name}.dn{far}"],
            sends=extra(far) if extra else [],
        )
        ends[far] = f"{name}.last"
        return [f"{name}.up1", f"{name}.dn1"], ends

    def scatter(name, axis, block, half, up_in, dn_in, half_in, rank, cost, ready, last, then=()):
        n, me, to = ring_at(axis)
        far = n // 2

        def idx(d):
            return (me + d + n) % n

        for j in range(1, far + 1):
            up, dn = idx(j), idx(-j)
            if j == far:
                su, tu = half(up, 0), half_in(up_in, j - 1, 0)
                sd, td = half(dn, 1), half_in(dn_in, j - 1, 1)
            else:
                su, tu, sd, td = block(up), up_in.at[j - 1], block(dn), dn_in.at[j - 1]
            plan.message(f"{name}.up{j}", axis + "+", su, tu, to(1), nbytes_of(su))
            plan.message(f"{name}.dn{j}", axis + "-", sd, td, to(-1), nbytes_of(sd))
        plan.task(
            f"{name}.start", rank, 0.02, after=ready(far), sends=[f"{name}.up{far}", f"{name}.dn{far}"]
        )
        for j in range(far - 1, 0, -1):
            for way, sign, h, came in (("up", 1, 0, up_in), ("dn", -1, 1, dn_in)):
                at = idx(sign * j)

                def add(at=at, j=j, h=h, came=came):
                    if j + 1 == far:
                        own, other = half(at, h), half_in(came, j, h)
                    else:
                        own, other = block(at), came.at[j]
                    own[...] = (own[...].astype(F32) + other[...].astype(F32)).astype(BF16)

                plan.task(
                    f"{name}.{way}{j}",
                    rank,
                    cost,
                    add,
                    waits=[f"{name}.{way}{j + 1}"],
                    after=ready(sign * j),
                    sends=[f"{name}.{way}{j}"],
                )
        own = block(me)

        def end():
            last(own[...].astype(F32) + up_in[0].astype(F32) + dn_in[0].astype(F32))

        plan.task(
            f"{name}.end",
            rank,
            cost * 1.5,
            end,
            waits=[f"{name}.up1", f"{name}.dn1"],
            after=ready(0),
            sends=then,
        )

    offsets_z = [0] + [s * h for h in range(1, nz // 2) for s in (-1, 1)] + [nz // 2]

    ax_first, ax_ends = gather(
        "wax", "x", lambda i: wa.at[z * nx + i], lambda i, h: wa.at[z * nx + i, pl.ds(h * shard // 2, shard // 2)], 0
    )
    az_first, az_ends = gather(
        "waz",
        "z",
        lambda i: wa.at[pl.ds(i * nx, nx)],
        lambda i, h: wa.at[pl.ds(i * nx + h * (nx // 2), nx // 2)],
        1,
    )
    plan.task("waz.go", 0, 0.02, after=[t for t in ax_ends.values() if t], sends=az_first)
    az_ends[0] = "waz.go"
    bx_first, bx_ends = {}, {}
    for d in offsets_z:
        bx_first[d], bx_ends[d] = gather(
            f"wbx{d}",
            "x",
            lambda i, d=d: wb.at[((z + d + nz) % nz) * nx + i],
            lambda i, h, d=d: wb.at[((z + d + nz) % nz) * nx + i, pl.ds(h * shard // 2, shard // 2)],
            2,
        )
    bz_first, bz_ends = gather(
        "wbz",
        "z",
        lambda i: wb.at[i * nx + x],
        lambda i, h: wb.at[i * nx + x, pl.ds(h * shard // 2, shard // 2)],
        0,
        extra=lambda d: bx_first[d],
    )

    def tok_at(i):
        return tok.at[pl.ds((i * NC + c) * mine, mine)]

    for d in range(-(ny // 2) + 1, ny // 2 + 1):
        block = tok_at((y + d + ny) % ny)
        plan.message(f"twin{d}", "twin", block, block, twin, nbytes_of(block))
    tok_first, tok_ends = gather(
        "tok",
        "y",
        tok_at,
        lambda i, h: tok.at[pl.ds((i * NC + c) * mine + h * (mine // 2), mine // 2)],
        0,
        extra=lambda d: [f"twin{d}"],
    )
    plan.task("tok.own", 0, 0.02, lambda: loads["tok"].wait(), sends=tok_first + ["twin0"])
    plan.task("go", -1, 0.02, sends=ax_first + bz_first + bx_first[0])
    plan.task(
        "tok.all",
        3,
        0.02,
        waits=[f"twin{d}" for d in range(-(ny // 2) + 1, ny // 2 + 1)],
        after=[t for t in tok_ends.values() if t] + ["tok.own"],
    )

    k0 = 0.7978845608028654
    k1 = k0 * 0.044715

    def act_step(row, col, size, write):
        r = pl.ds(row, SUB)
        cols = pl.ds(col, size)
        g = gate[r, cols].astype(F32)
        before = gate[pl.ds(pl.multiple_of(jnp.maximum(row - 16, 0), 16), 16), cols].astype(F32)[8:]
        before = jnp.where(row > 0, before, 0.0)
        both = jnp.concatenate([before, g], axis=0)
        one = pltpu.roll(both, 1, 0)[8:]
        two = pltpu.roll(both, 2, 0)[8:]
        w0, w1, w2 = cw[0:1, cols], cw[1:2, cols], cw[2:3, cols]
        conv = cb[0:1, cols] + w0 * two + w1 * one + w2 * g
        square = conv * conv
        t = jnp.tanh(conv * (k0 + k1 * square))
        cdf = 0.5 + 0.5 * t
        slope = cdf + conv * (0.5 - 0.5 * (t * t)) * (k0 + (3.0 * k1) * square)
        hg = hidden[r, cols].astype(F32)
        vg = hg * (conv * cdf)
        cg = slope * (hg * value[r, cols].astype(F32))
        after = jnp.concatenate([cg, later[:, cols]], axis=0)
        gg = (
            w2 * cg
            + w1 * pltpu.roll(after, SUB + 7, 0)[:SUB]
            + w0 * pltpu.roll(after, SUB + 6, 0)[:SUB]
        )
        later[:, cols] = cg[:8]
        for k, term in enumerate((cg * two, cg * one, cg * g, cg)):
            terms[k, :, cols] += term.reshape(SUB // 8, 8, size).sum(axis=0)
        write(r, cols, gg, vg)

    def write_whole(r, cols, gg, vg):
        ga[r, cols] = gg.astype(BF16)
        gb[r, cols] = vg.astype(BF16)

    def write_rest(r, cols, gg, vg):
        gb[r, whole:] = jnp.concatenate([vg, gg], axis=1).astype(BF16)

    n_act = 8 if rows >= 8 * SUB else rows // SUB
    per_act = rows // n_act // SUB

    def act(k):
        if k == 0:
            for name in ("gate", "value", "hidden", "cw", "cb"):
                loads[name].wait()

        def sub(i, carry):
            row = pl.multiple_of(rows - (k * per_act + i + 1) * SUB, SUB)

            def col(j, carry):
                act_step(row, pl.multiple_of(j * LANES, LANES), LANES, write_whole)
                return carry

            lax.fori_loop(0, whole // LANES, col, 0)
            act_step(row, whole, rest, write_rest)
            return carry

        lax.fori_loop(0, per_act, sub, 0)

    for k in range(n_act):
        plan.task(f"act{k}", 5, 1.1, functools.partial(act, k), after=[f"act{k - 1}"] if k else [])
    acted = f"act{n_act - 1}"

    def conv_start():
        sums = [terms[k].sum(axis=0, keepdims=True) for k in range(4)]
        cx[x] = jnp.concatenate(sums + [jnp.zeros((4, width), F32)], axis=0)

    def ring_of_slots(name, axis, slots):
        n, me, to = ring_at(axis)
        names = []
        for h in range(1, n // 2 + 1):
            for way, sign in (("up", 1), ("dn", -1)):
                if h == n // 2 and sign < 0:
                    continue
                s = slots.at[(me + sign * (1 - h) + n) % n]
                m = f"{name}.{way}{h}"
                plan.message(m, axis + ("+" if sign > 0 else "-"), s, s, to(sign), nbytes_of(s))
                nxt = [f"{name}.{way}{h + 1}"] if h + 1 < n // 2 or (h + 1 == n // 2 and sign > 0) else []
                plan.task(m, 4, 0.05, waits=[m], sends=nxt)
                names.append(m)
        firsts = [f"{name}.up1"] + ([f"{name}.dn1"] if n > 2 else [])
        return firsts, names

    cx_first, cx_names = ring_of_slots("cx", "x", cx)
    cz_first, cz_names = ring_of_slots("cz", "z", cz)

    def conv_middle():
        total = cx[0]
        for i in range(1, nx):
            total = total + cx[i]
        cz[z] = total

    def conv_end():
        total = cz[0]
        for i in range(1, nz):
            total = total + cz[i]
        total = total * scale
        cwg_out[...] = total[:3]
        cbg_out[...] = total[3:4]

    plan.task("conv.start", 6, 0.2, conv_start, after=[acted], sends=cx_first)
    plan.task("conv.middle", 6, 0.1, conv_middle, after=cx_names + ["conv.start"], sends=cz_first)
    plan.task("conv.end", 9, 0.1, conv_end, after=cz_names + ["conv.middle"])

    grad_order = [nz // 2] + [s * h for h in range(nz // 2 - 1, 0, -1) for s in (1, -1)] + [0]

    def grad(d):
        to_z = (z + d + nz) % nz
        left = tok[:, pl.ds(pl.multiple_of(to_z * group, group), group)]
        over_rows = (((0,), (0,)), ((), ()))
        for right, out in ((ga, pa), (gb, pb)):
            part = lax.dot_general(left, right[...], over_rows, preferred_element_type=F32)
            out[to_z] = part.astype(BF16).reshape(nx, shard, part.shape[1])

    for d in grad_order:
        plan.task(f"grad{d}", 7, 1.1, functools.partial(grad, d), after=["tok.all", acted])

    def ax_last(total):
        gg_out[:, :whole] = total * scale

    def az_last(total):
        pa[z] = total.astype(BF16)

    scatter(
        "pax",
        "x",
        lambda i: pa.at[z, i],
        lambda i, h: pa.at[z, i, pl.ds(h * shard // 2, shard // 2)],
        ax_up,
        ax_dn,
        lambda ref, j, h: ref.at[j, pl.ds(h * shard // 2, shard // 2)],
        3,
        0.1,
        lambda d: ["paz.end"],
        ax_last,
    )
    scatter(
        "paz",
        "z",
        lambda i: pa.at[i],
        lambda i, h: pa.at[i, pl.ds(h * (nx // 2), nx // 2)],
        az_up,
        az_dn,
        lambda ref, j, h: ref.at[j, pl.ds(h * (nx // 2), nx // 2)],
        2,
        0.25,
        lambda d: [f"grad{d}"],
        az_last,
    )

    def bz_last(total):
        total = total * scale
        vg_out[...] = total[:, :width]
        gg_out[:, whole:] = total[:, width:]

    def bx_last(d, total):
        pb[(z + d + nz) % nz, x] = total.astype(BF16)

    for i, d in enumerate(grad_order):
        scatter(
            f"pbx{d}",
            "x",
            lambda i, d=d: pb.at[(z + d + nz) % nz, i],
            lambda i, h, d=d: pb.at[(z + d + nz) % nz, i, pl.ds(h * shard // 2, shard // 2)],
            bx_up.at[i],
            bx_dn.at[i],
            lambda ref, j, h: ref.at[j, pl.ds(h * shard // 2, shard // 2)],
            2,
            0.1,
            lambda e, d=d: [f"grad{d}"],
            functools.partial(bx_last, d),
        )
    scatter(
        "pbz",
        "z",
        lambda i: pb.at[i, x],
        lambda i, h: pb.at[i, x, pl.ds(h * shard // 2, shard // 2)],
        bz_up,
        bz_dn,
        lambda ref, j, h: ref.at[j, pl.ds(h * shard // 2, shard // 2)],
        2,
        0.1,
        lambda d: [f"pbx{d}.end"],
        bz_last,
    )

    over_cols = (((1,), (1,)), ((), ()))

    def ig(d):
        at = (z + d + nz) % nz
        left_w = wa[pl.ds(at * nx, nx)].reshape(group, whole)
        right_w = wb[pl.ds(at * nx, nx)].reshape(group, 2 * width - whole)
        part = lax.dot_general(ga[...], left_w, over_cols, preferred_element_type=F32)
        part = part + lax.dot_general(gb[...], right_w, over_cols, preferred_element_type=F32)
        part = part.astype(BF16)
        for k in range(ny * NC):
            igp[at, k % NC, k // NC] = part[k * mine : (k + 1) * mine]

    for d in offsets_z:
        at = (z + d + nz) % nz
        m = f"igt{d}"
        source, target = igp.at[at, 1 - c], twin_in.at[at]
        plan.message(m, "twin", source, target, twin, nbytes_of(source))
        ends = [t for t in (az_ends[d], bz_ends[d], *bx_ends[d].values()) if t]
        plan.task(f"ig{d}", 8, 1.1, functools.partial(ig, d), after=[acted] + ends, sends=[m])

        def merge(at=at):
            igp[at, c] = (igp[at, c].astype(F32) + twin_in[at].astype(F32)).astype(BF16)

        plan.task(f"igm{d}", 3, 0.2, merge, waits=[m], after=[f"ig{d}"])

        def ig_last(total, at=at):
            ig_out[:, pl.ds(pl.multiple_of(at * group, group), group)] = total.astype(BF16)

        scatter(
            f"igy{d}",
            "y",
            lambda i, at=at: igp.at[at, c, i],
            lambda i, h, at=at: igp.at[at, c, i, pl.ds(h * (mine // 2), mine // 2)],
            y_up.at[at],
            y_dn.at[at],
            lambda ref, j, h: ref.at[j, pl.ds(h * (mine // 2), mine // 2)],
            3,
            0.05,
            lambda e, d=d: [f"igm{d}"],
            ig_last,
        )

    copies = {}
    number = {name: i for i, name in enumerate(plan.messages)}
    for name, (link, source, target, device, size) in plan.messages.items():
        i = number[name]
        copies[name] = pltpu.make_async_remote_copy(
            src_ref=source,
            dst_ref=target,
            send_sem=send_sem.at[i],
            recv_sem=recv_sem.at[i],
            device_id=device,
            device_id_type=MESH,
        )
    for name in plan.order():
        rank, cost, body, waits, after, sends = plan.tasks[name]
        for m in waits:
            copies[m].wait_recv()
        if body is not None:
            body()
        for m in sends:
            copies[m].start()
    for m in plan.messages:
        copies[m].wait_send()


def on_device(dims, *args):
    tokens, gate_pre, value_pre, up_gate_w, up_value_w, conv_weight, conv_bias, hidden_grad = args
    nz, nx, ny = dims
    rows, width = gate_pre.shape
    mine, model = tokens.shape
    shard = up_gate_w.shape[0]
    whole = width // LANES * LANES
    ca, cb = whole, 2 * width - whole
    group = nx * shard
    shape = jax.ShapeDtypeStruct
    out = pl.pallas_call(
        functools.partial(kernel, dims),
        out_shape=(
            shape((mine, model), BF16),
            shape((shard, width), F32),
            shape((shard, width), F32),
            shape((3, width), F32),
            shape((1, width), F32),
        ),
        in_specs=[pl.BlockSpec(memory_space=pl.ANY)] * 8,
        out_specs=[pl.BlockSpec(memory_space=pltpu.VMEM)] * 5,
        scratch_shapes=[
            pltpu.VMEM((rows, width), BF16),
            pltpu.VMEM((rows, width), BF16),
            pltpu.VMEM((rows, width), BF16),
            pltpu.VMEM((shard, width), BF16),
            pltpu.VMEM((shard, width), BF16),
            pltpu.VMEM((3, width), F32),
            pltpu.VMEM((1, width), F32),
            pltpu.VMEM((mine * ny * NC, model), BF16),
            pltpu.VMEM((nz * nx, shard, ca), BF16),
            pltpu.VMEM((nz * nx, shard, cb), BF16),
            pltpu.VMEM((rows, ca), BF16),
            pltpu.VMEM((rows, cb), BF16),
            pltpu.VMEM((nz, nx, shard, ca), BF16),
            pltpu.VMEM((nz, nx, shard, cb), BF16),
            pltpu.VMEM((nz // 2, nx, shard, ca), BF16),
            pltpu.VMEM((nz // 2, nx, shard, ca), BF16),
            pltpu.VMEM((nx // 2, shard, ca), BF16),
            pltpu.VMEM((nx // 2, shard, ca), BF16),
            pltpu.VMEM((nz, nx // 2, shard, cb), BF16),
            pltpu.VMEM((nz, nx // 2, shard, cb), BF16),
            pltpu.VMEM((nz // 2, shard, cb), BF16),
            pltpu.VMEM((nz // 2, shard, cb), BF16),
            pltpu.VMEM((nz, NC, ny, mine, group), BF16),
            pltpu.VMEM((nz, ny, mine, group), BF16),
            pltpu.VMEM((nz, ny // 2, mine, group), BF16),
            pltpu.VMEM((nz, ny // 2, mine, group), BF16),
            pltpu.VMEM((8, width), F32),
            pltpu.VMEM((4, 8, width), F32),
            pltpu.VMEM((nx, 8, width), F32),
            pltpu.VMEM((nz, 8, width), F32),
            pltpu.SemaphoreType.DMA((8,)),
            pltpu.SemaphoreType.DMA((192,)),
            pltpu.SemaphoreType.DMA((192,)),
        ],
        compiler_params=pltpu.CompilerParams(
            collective_id=0, has_side_effects=True, vmem_limit_bytes=64_000_000
        ),
    )(
        tokens,
        gate_pre,
        value_pre,
        up_gate_w,
        up_value_w,
        conv_weight,
        conv_bias.reshape(1, width),
        hidden_grad,
    )
    return (out[0], out[1], out[2], out[3], out[4].reshape(width))


def solution(mesh):
    sizes = (mesh.shape["fs"], mesh.shape["tp"])
    dims = {(32, 8): (8, 4, 4)}[sizes]
    in_specs = (
        P(("fs", "tp"), None),
        P("fs", "tp"),
        P("fs", "tp"),
        P("fs", "tp"),
        P("fs", "tp"),
        P(None, "tp"),
        P("tp"),
        P("fs", "tp"),
    )
    out_specs = (P(("fs", "tp"), None), P("fs", "tp"), P("fs", "tp"), P(None, "tp"), P("tp"))
    return jax.shard_map(
        functools.partial(on_device, dims),
        mesh=mesh,
        in_specs=in_specs,
        out_specs=out_specs,
        check_vma=False,
    )
```

```python
import functools

import jax
import jax.numpy as jnp
from jax import lax
from jax.experimental import pallas as pl
from jax.experimental.pallas import tpu as pltpu
from jax.sharding import PartitionSpec as P

MESH = pl.DeviceIdType.MESH
F32 = jnp.float32
BF16 = jnp.bfloat16
NC = 2
SUB = 16
LANES = 128

LINK = 46_650.0
TWIN = 300_000.0
HOP = 2.2
TWIN_HOP = 1.0


class Plan:
    def __init__(self):
        self.messages = {}
        self.tasks = {}

    def message(self, name, link, source, target, device, nbytes):
        self.messages[name] = (link, source, target, device, nbytes)

    def task(self, name, rank, cost, body=None, waits=(), after=(), sends=()):
        self.tasks[name] = (rank, cost, body, tuple(waits), tuple(after), tuple(sends))

    def order(self):
        arrival, free, ended, listed = {}, {}, {}, []
        left = dict(self.tasks)
        now = 0.0
        while left:
            best = None
            for name, (rank, cost, body, waits, after, sends) in left.items():
                if any(w not in arrival for w in waits) or any(a not in ended for a in after):
                    continue
                ready = max([now] + [arrival[w] for w in waits])
                key = (ready > now, ready if ready > now else 0.0, rank)
                if best is None or key < best[0]:
                    best = (key, name, ready)
            name, ready = best[1], best[2]
            rank, cost, body, waits, after, sends = left.pop(name)
            now = ready + cost
            ended[name] = now
            listed.append(name)
            for m in sends:
                link, nbytes = self.messages[m][0], self.messages[m][4]
                start = max(now, free.get(link, 0.0))
                rate, hop = (TWIN, TWIN_HOP) if link == "twin" else (LINK, HOP)
                free[link] = start + nbytes / rate
                arrival[m] = free[link] + hop
        self.length = now
        self.ended = ended
        return listed


def nbytes_of(ref):
    size = ref.dtype.itemsize
    for s in ref.shape:
        size *= s
    return size


def kernel(
    dims,
    tokens,
    gate_in,
    value_in,
    wg_in,
    wv_in,
    cw_in,
    cb_in,
    hidden_in,
    ig_out,
    gg_out,
    vg_out,
    cwg_out,
    cbg_out,
    gate,
    value,
    hidden,
    wgs,
    wvs,
    cw,
    cb,
    tok,
    wa,
    wb,
    gt,
    pa,
    pb,
    az_up,
    az_dn,
    ax_up,
    ax_dn,
    bx_up,
    bx_dn,
    bz_up,
    bz_dn,
    igp,
    twin_in,
    y_up,
    y_dn,
    taps,
    coef,
    terms,
    cx,
    cz,
    load_sem,
    send_sem,
    recv_sem,
):
    nz, nx, ny = dims
    fs, tp = lax.axis_index("fs"), lax.axis_index("tp")
    z, x, y, c = fs // nx, fs % nx, tp // NC, tp % NC
    width, rows = gate.shape
    mine = tok.shape[0] // (ny * NC)
    whole = width // LANES * LANES
    rest = width - whole
    ahead = pa.shape[3]
    shard = wgs.shape[0]
    group = nx * shard
    scale = float(rows * nz * nx) ** (-0.5)

    def at_z(d):
        return (((z + d + nz) % nz) * nx + x, tp)

    def at_x(d):
        return (z * nx + (x + d + nx) % nx, tp)

    def at_y(d):
        return (fs, ((y + d + ny) % ny) * NC + c)

    twin = (fs, y * NC + 1 - c)

    loads = {}
    for i, (name, source, target) in enumerate(
        (
            ("wg", wg_in, wgs),
            ("wv", wv_in, wvs),
            ("tok", tokens, tok.at[pl.ds(tp * mine, mine)]),
            ("gate", gate_in, gate),
            ("value", value_in, value),
            ("hidden", hidden_in, hidden),
            ("cw", cw_in, cw),
            ("cb", cb_in, cb),
        )
    ):
        loads[name] = pltpu.make_async_copy(source, target, load_sem.at[i])
        loads[name].start()
    barrier = pltpu.get_barrier_semaphore()
    peers = (at_z(1), at_z(-1), at_x(1), at_x(-1), at_y(1), at_y(-1), twin)
    for peer in peers:
        pl.semaphore_signal(barrier, inc=1, device_id=peer, device_id_type=MESH)

    loads["wg"].wait()
    loads["wv"].wait()
    wa[fs] = wgs[:, :whole]
    wb[fs, :, :whole] = wvs[:, :whole]
    wb[fs, :, whole:] = jnp.concatenate(
        [wvs[:, whole:].astype(F32), wgs[:, whole:].astype(F32)], axis=1
    ).astype(BF16)
    terms[:, width:] = jnp.zeros((4, terms.shape[1] - width, LANES), F32)
    pl.semaphore_wait(barrier, len(peers))

    plan = Plan()

    def ring_at(axis):
        return {
            "z": (nz, z, at_z),
            "x": (nx, x, at_x),
            "y": (ny, y, at_y),
        }[axis]

    def gather(name, axis, block, half, rank, extra=None, first=None):
        n, me, to = ring_at(axis)
        far = n // 2

        def idx(d):
            return (me + d + n) % n

        for h in range(1, far + 1):
            up, dn = idx(1 - h), idx(h - 1)
            su, sd = (block(up), block(dn)) if h < far else (half(up, 0), half(dn, 1))
            plan.message(f"{name}.up{h}", axis + "+", su, su, to(1), nbytes_of(su))
            plan.message(f"{name}.dn{h}", axis + "-", sd, sd, to(-1), nbytes_of(sd))
        ends = {0: first}
        for h in range(1, far):
            for way, sign in (("up", -1), ("dn", 1)):
                task = f"{name}.{way}{h}"
                plan.task(
                    task,
                    rank,
                    0.05,
                    waits=[task],
                    sends=[f"{name}.{way}{h + 1}"] + (extra(sign * h) if extra else []),
                )
                ends[sign * h] = task
        plan.task(
            f"{name}.last",
            rank,
            0.05,
            waits=[f"{name}.up{far}", f"{name}.dn{far}"],
            sends=extra(far) if extra else [],
        )
        ends[far] = f"{name}.last"
        return [f"{name}.up1", f"{name}.dn1"], ends

    def scatter(name, axis, block, half, up_in, dn_in, half_in, rank, cost, ready, last, then=()):
        n, me, to = ring_at(axis)
        far = n // 2

        def idx(d):
            return (me + d + n) % n

        for j in range(1, far + 1):
            up, dn = idx(j), idx(-j)
            if j == far:
                su, tu = half(up, 0), half_in(up_in, j - 1, 0)
                sd, td = half(dn, 1), half_in(dn_in, j - 1, 1)
            else:
                su, tu, sd, td = block(up), up_in.at[j - 1], block(dn), dn_in.at[j - 1]
            plan.message(f"{name}.up{j}", axis + "+", su, tu, to(1), nbytes_of(su))
            plan.message(f"{name}.dn{j}", axis + "-", sd, td, to(-1), nbytes_of(sd))
        plan.task(
            f"{name}.start", rank, 0.02, after=ready(far), sends=[f"{name}.up{far}", f"{name}.dn{far}"]
        )
        for j in range(far - 1, 0, -1):
            for way, sign, h, came in (("up", 1, 0, up_in), ("dn", -1, 1, dn_in)):
                at = idx(sign * j)

                def add(at=at, j=j, h=h, came=came):
                    if j + 1 == far:
                        own, other = half(at, h), half_in(came, j, h)
                    else:
                        own, other = block(at), came.at[j]
                    own[...] = (own[...].astype(F32) + other[...].astype(F32)).astype(BF16)

                plan.task(
                    f"{name}.{way}{j}",
                    rank,
                    cost,
                    add,
                    waits=[f"{name}.{way}{j + 1}"],
                    after=ready(sign * j),
                    sends=[f"{name}.{way}{j}"],
                )
        own = block(me)

        def end():
            last(own[...].astype(F32) + up_in[0].astype(F32) + dn_in[0].astype(F32))

        plan.task(
            f"{name}.end",
            rank,
            cost * 1.5,
            end,
            waits=[f"{name}.up1", f"{name}.dn1"],
            after=ready(0),
            sends=then,
        )

    offsets_z = [0] + [s * h for h in range(1, nz // 2) for s in (-1, 1)] + [nz // 2]

    offsets_x = [0] + [s * h for h in range(1, nx // 2) for s in (-1, 1)] + [nx // 2]
    az_first, az_ends = {}, {}
    for r in offsets_x:
        col = (x + r + nx) % nx
        az_first[r], az_ends[r] = gather(
            f"waz{r}",
            "z",
            lambda i, col=col: wa.at[i * nx + col],
            lambda i, h, col=col: wa.at[i * nx + col, pl.ds(h * shard // 2, shard // 2)],
            1,
        )
    ax_first, ax_ends = gather(
        "wax",
        "x",
        lambda i: wa.at[z * nx + i],
        lambda i, h: wa.at[z * nx + i, pl.ds(h * shard // 2, shard // 2)],
        0,
        extra=lambda r: az_first[r],
    )
    for r in offsets_x:
        az_ends[r][0] = ax_ends[r]
    bx_first, bx_ends = {}, {}
    for d in offsets_z:
        bx_first[d], bx_ends[d] = gather(
            f"wbx{d}",
            "x",
            lambda i, d=d: wb.at[((z + d + nz) % nz) * nx + i],
            lambda i, h, d=d: wb.at[((z + d + nz) % nz) * nx + i, pl.ds(h * shard // 2, shard // 2)],
            2,
        )
    bz_first, bz_ends = gather(
        "wbz",
        "z",
        lambda i: wb.at[i * nx + x],
        lambda i, h: wb.at[i * nx + x, pl.ds(h * shard // 2, shard // 2)],
        0,
        extra=lambda d: bx_first[d],
    )

    def tok_at(i):
        return tok.at[pl.ds((i * NC + c) * mine, mine)]

    for d in range(-(ny // 2) + 1, ny // 2 + 1):
        block = tok_at((y + d + ny) % ny)
        plan.message(f"twin{d}", "twin", block, block, twin, nbytes_of(block))
    tok_first, tok_ends = gather(
        "tok",
        "y",
        tok_at,
        lambda i, h: tok.at[pl.ds((i * NC + c) * mine + h * (mine // 2), mine // 2)],
        0,
        extra=lambda d: [f"twin{d}"],
    )
    plan.task("tok.own", 0, 0.02, lambda: loads["tok"].wait(), sends=tok_first + ["twin0"])
    plan.task("go", -1, 0.02, sends=ax_first + bz_first + bx_first[0] + az_first[0])
    plan.task(
        "tok.all",
        3,
        0.02,
        waits=[f"twin{d}" for d in range(-(ny // 2) + 1, ny // 2 + 1)],
        after=[t for t in tok_ends.values() if t] + ["tok.own"],
    )

    k0 = 0.7978845608028654
    k1 = k0 * 0.044715

    lane = lax.broadcasted_iota(jnp.int32, (SUB, LANES), 1)

    def shifted(value, by):
        turned = pltpu.roll(value, by % rows, 1)
        if by > 0:
            edge = jnp.where(lane < by, 0.0, turned[:, :LANES])
            return jnp.concatenate([edge, turned[:, LANES:]], axis=1)
        edge = jnp.where(lane >= LANES + by, 0.0, turned[:, rows - LANES :])
        return jnp.concatenate([turned[:, : rows - LANES], edge], axis=1)

    def act_step(i):
        units = pl.ds(pl.multiple_of(i * SUB, SUB), SUB)
        g = gate[units, :].astype(F32)
        one, two = shifted(g, 1), shifted(g, 2)
        w0, w1, w2 = coef[units, 0:1], coef[units, 1:2], coef[units, 2:3]
        conv = coef[units, 3:4] + w0 * two + w1 * one + w2 * g
        square = conv * conv
        t = jnp.tanh(conv * (k0 + k1 * square))
        cdf = 0.5 + 0.5 * t
        slope = cdf + conv * (0.5 - 0.5 * (t * t)) * (k0 + (3.0 * k1) * square)
        hg = hidden[units, :].astype(F32)
        cg = slope * (hg * value[units, :].astype(F32))
        gg = w2 * cg + w1 * shifted(cg, -1) + w0 * shifted(cg, -2)
        for k, term in enumerate((cg * two, cg * one, cg * g, cg)):
            total = term[:, :LANES]
            for j in range(1, rows // LANES):
                total = total + term[:, j * LANES : (j + 1) * LANES]
            terms[k, units, :] = total
        at = jnp.where(i * SUB < whole, i * SUB, i * SUB + width)
        gt[pl.ds(pl.multiple_of(at, SUB), SUB), :] = gg.astype(BF16)
        at = i * SUB + whole
        gt[pl.ds(pl.multiple_of(at, SUB), SUB), :] = (hg * (conv * cdf)).astype(BF16)

    n_act = 11
    per_act = width // SUB // n_act

    def act(k):
        if k == 0:
            for name in ("gate", "value", "hidden", "cw", "cb"):
                loads[name].wait()
            taps[0:3, :width] = cw[...]
            taps[3, :width] = cb[...]
            coef[...] = taps[...].T

        def step(i, carry):
            act_step(k * per_act + i)
            return carry

        lax.fori_loop(0, per_act, step, 0)

    for k in range(n_act):
        plan.task(f"act{k}", 5, 0.8, functools.partial(act, k), after=[f"act{k - 1}"] if k else [])
    acted = f"act{n_act - 1}"

    pad = taps.shape[1]

    def conv_start():
        sums = jnp.concatenate([terms[k].T.sum(axis=0, keepdims=True) for k in range(4)], axis=0)
        cx[x] = jnp.concatenate([sums[:, : pad // 2], sums[:, pad // 2 :]], axis=0)

    def ring_of_slots(name, axis, slots):
        n, me, to = ring_at(axis)
        names = []
        for h in range(1, n // 2 + 1):
            for way, sign in (("up", 1), ("dn", -1)):
                if h == n // 2 and sign < 0:
                    continue
                s = slots.at[(me + sign * (1 - h) + n) % n]
                m = f"{name}.{way}{h}"
                plan.message(m, axis + ("+" if sign > 0 else "-"), s, s, to(sign), nbytes_of(s))
                nxt = [f"{name}.{way}{h + 1}"] if h + 1 < n // 2 or (h + 1 == n // 2 and sign > 0) else []
                plan.task(m, 4, 0.05, waits=[m], sends=nxt)
                names.append(m)
        firsts = [f"{name}.up1"] + ([f"{name}.dn1"] if n > 2 else [])
        return firsts, names

    cx_first, cx_names = ring_of_slots("cx", "x", cx)
    cz_first, cz_names = ring_of_slots("cz", "z", cz)

    def conv_middle():
        total = cx[0]
        for i in range(1, nx):
            total = total + cx[i]
        cz[z] = total

    def conv_end():
        total = cz[0]
        for i in range(1, nz):
            total = total + cz[i]
        total = total * scale
        total = jnp.concatenate([total[:4], total[4:]], axis=1)[:, :width]
        cwg_out[...] = total[:3]
        cbg_out[...] = total[3]

    plan.task("conv.start", 6, 0.2, conv_start, after=[acted], sends=cx_first)
    plan.task("conv.middle", 6, 0.1, conv_middle, after=cx_names + ["conv.start"], sends=cz_first)
    plan.task("conv.end", 9, 0.1, conv_end, after=cz_names + ["conv.middle"])

    grad_order = [nz // 2] + [s * h for h in range(nz // 2 - 1, 0, -1) for s in (1, -1)] + [0]

    def grad(d):
        to_z = (z + d + nz) % nz
        left = tok[:, pl.ds(pl.multiple_of(to_z * group, group), group)]
        over_rows = (((0,), (1,)), ((), ()))
        for right, out in ((gt.at[:ahead], pa), (gt.at[ahead:], pb)):
            part = lax.dot_general(left, right[...], over_rows, preferred_element_type=F32)
            out[to_z] = part.astype(BF16).reshape(nx, shard, part.shape[1])

    for d in grad_order:
        plan.task(f"grad{d}", 7, 1.1, functools.partial(grad, d), after=["tok.all", acted])

    def ax_last(total):
        gg_out[:, :ahead] = total * scale

    def az_last(r, total):
        pa[z, (x + r + nx) % nx] = total.astype(BF16)

    scatter(
        "pax",
        "x",
        lambda i: pa.at[z, i],
        lambda i, h: pa.at[z, i, pl.ds(h * shard // 2, shard // 2)],
        ax_up,
        ax_dn,
        lambda ref, j, h: ref.at[j, pl.ds(h * shard // 2, shard // 2)],
        3,
        0.1,
        lambda d: [f"paz{d}.end"],
        ax_last,
    )
    for i, r in enumerate([nx // 2] + [s * h for h in range(nx // 2 - 1, 0, -1) for s in (1, -1)] + [0]):
        col = (x + r + nx) % nx
        scatter(
            f"paz{r}",
            "z",
            lambda i, col=col: pa.at[i, col],
            lambda i, h, col=col: pa.at[i, col, pl.ds(h * shard // 2, shard // 2)],
            az_up.at[i],
            az_dn.at[i],
            lambda ref, j, h: ref.at[j, pl.ds(h * shard // 2, shard // 2)],
            2,
            0.1,
            lambda d: [f"grad{d}"],
            functools.partial(az_last, r),
        )

    def bz_last(total):
        total = total * scale
        start = whole - ahead
        gg_out[:, ahead:whole] = total[:, :start]
        vg_out[...] = total[:, start : start + width]
        gg_out[:, whole:] = total[:, start + width :]

    def bx_last(d, total):
        pb[(z + d + nz) % nz, x] = total.astype(BF16)

    for i, d in enumerate(grad_order):
        scatter(
            f"pbx{d}",
            "x",
            lambda i, d=d: pb.at[(z + d + nz) % nz, i],
            lambda i, h, d=d: pb.at[(z + d + nz) % nz, i, pl.ds(h * shard // 2, shard // 2)],
            bx_up.at[i],
            bx_dn.at[i],
            lambda ref, j, h: ref.at[j, pl.ds(h * shard // 2, shard // 2)],
            2,
            0.1,
            lambda e, d=d: [f"grad{d}"],
            functools.partial(bx_last, d),
        )
    scatter(
        "pbz",
        "z",
        lambda i: pb.at[i, x],
        lambda i, h: pb.at[i, x, pl.ds(h * shard // 2, shard // 2)],
        bz_up,
        bz_dn,
        lambda ref, j, h: ref.at[j, pl.ds(h * shard // 2, shard // 2)],
        2,
        0.1,
        lambda d: [f"pbx{d}.end"],
        bz_last,
    )


    def ig(d):
        at = (z + d + nz) % nz
        left_w = wa[pl.ds(at * nx, nx)].reshape(group, whole)
        right_w = wb[pl.ds(at * nx, nx)].reshape(group, 2 * width - whole)
        part = jnp.dot(left_w, gt[:whole], preferred_element_type=F32)
        part = part + jnp.dot(right_w, gt[whole:], preferred_element_type=F32)
        part = part.astype(BF16)
        for k in range(ny * NC):
            igp[at, k % NC, k // NC] = part[:, k * mine : (k + 1) * mine]

    for d in offsets_z:
        at = (z + d + nz) % nz
        m = f"igt{d}"
        source, target = igp.at[at, 1 - c], twin_in.at[at]
        plan.message(m, "twin", source, target, twin, nbytes_of(source))
        ends = [a[d] for a in az_ends.values()] + [bz_ends[d], *bx_ends[d].values()]
        ends = [t for t in ends if t]
        plan.task(f"ig{d}", 8, 1.1, functools.partial(ig, d), after=[acted] + ends, sends=[m])

        def merge(at=at):
            igp[at, c] = (igp[at, c].astype(F32) + twin_in[at].astype(F32)).astype(BF16)

        plan.task(f"igm{d}", 3, 0.2, merge, waits=[m], after=[f"ig{d}"])

        def ig_last(total, at=at):
            ig_out[:, pl.ds(pl.multiple_of(at * group, group), group)] = total.T.astype(BF16)

        scatter(
            f"igy{d}",
            "y",
            lambda i, at=at: igp.at[at, c, i],
            lambda i, h, at=at: igp.at[at, c, i, pl.ds(h * (group // 2), group // 2)],
            y_up.at[at],
            y_dn.at[at],
            lambda ref, j, h: ref.at[j, pl.ds(h * (group // 2), group // 2)],
            3,
            0.05,
            lambda e, d=d: [f"igm{d}"],
            ig_last,
        )

    copies = {}
    number = {name: i for i, name in enumerate(plan.messages)}
    for name, (link, source, target, device, size) in plan.messages.items():
        i = number[name]
        copies[name] = pltpu.make_async_remote_copy(
            src_ref=source,
            dst_ref=target,
            send_sem=send_sem.at[i],
            recv_sem=recv_sem.at[i],
            device_id=device,
            device_id_type=MESH,
        )
    for name in plan.order():
        rank, cost, body, waits, after, sends = plan.tasks[name]
        for m in waits:
            copies[m].wait_recv()
        if body is not None:
            body()
        for m in sends:
            copies[m].start()
    for m in plan.messages:
        copies[m].wait_send()


def on_device(dims, *args):
    tokens, gate_pre, value_pre, up_gate_w, up_value_w, conv_weight, conv_bias, hidden_grad = args
    nz, nx, ny = dims
    rows, width = gate_pre.shape
    mine, model = tokens.shape
    shard = up_gate_w.shape[0]
    whole = width // LANES * LANES
    ca, cb = whole, 2 * width - whole
    pa, pb = whole - LANES, 2 * width - whole + LANES
    pad = whole + LANES
    group = nx * shard
    shape = jax.ShapeDtypeStruct
    return pl.pallas_call(
        functools.partial(kernel, dims),
        out_shape=(
            shape((mine, model), BF16),
            shape((shard, width), F32),
            shape((shard, width), F32),
            shape((3, width), F32),
            shape((width,), F32),
        ),
        in_specs=[pl.BlockSpec(memory_space=pl.ANY)] * 8,
        out_specs=[pl.BlockSpec(memory_space=pltpu.VMEM)] * 5,
        scratch_shapes=[
            pltpu.VMEM((width, rows), BF16),
            pltpu.VMEM((width, rows), BF16),
            pltpu.VMEM((width, rows), BF16),
            pltpu.VMEM((shard, width), BF16),
            pltpu.VMEM((shard, width), BF16),
            pltpu.VMEM((3, width), F32),
            pltpu.VMEM((width,), F32),
            pltpu.VMEM((mine * ny * NC, model), BF16),
            pltpu.VMEM((nz * nx, shard, ca), BF16),
            pltpu.VMEM((nz * nx, shard, cb), BF16),
            pltpu.VMEM((2 * width, rows), BF16),
            pltpu.VMEM((nz, nx, shard, pa), BF16),
            pltpu.VMEM((nz, nx, shard, pb), BF16),
            pltpu.VMEM((nx, nz // 2, shard, pa), BF16),
            pltpu.VMEM((nx, nz // 2, shard, pa), BF16),
            pltpu.VMEM((nx // 2, shard, pa), BF16),
            pltpu.VMEM((nx // 2, shard, pa), BF16),
            pltpu.VMEM((nz, nx // 2, shard, pb), BF16),
            pltpu.VMEM((nz, nx // 2, shard, pb), BF16),
            pltpu.VMEM((nz // 2, shard, pb), BF16),
            pltpu.VMEM((nz // 2, shard, pb), BF16),
            pltpu.VMEM((nz, NC, ny, group, mine), BF16),
            pltpu.VMEM((nz, ny, group, mine), BF16),
            pltpu.VMEM((nz, ny // 2, group, mine), BF16),
            pltpu.VMEM((nz, ny // 2, group, mine), BF16),
            pltpu.VMEM((8, pad), F32),
            pltpu.VMEM((pad, 8), F32),
            pltpu.VMEM((4, pad, LANES), F32),
            pltpu.VMEM((nx, 8, pad // 2), F32),
            pltpu.VMEM((nz, 8, pad // 2), F32),
            pltpu.SemaphoreType.DMA((8,)),
            pltpu.SemaphoreType.DMA((224,)),
            pltpu.SemaphoreType.DMA((224,)),
        ],
        compiler_params=pltpu.CompilerParams(
            collective_id=0, has_side_effects=True, vmem_limit_bytes=64_000_000
        ),
    )(
        tokens,
        gate_pre.T,
        value_pre.T,
        up_gate_w,
        up_value_w,
        conv_weight,
        conv_bias,
        hidden_grad.T,
    )


def solution(mesh):
    sizes = (mesh.shape["fs"], mesh.shape["tp"])
    dims = {(32, 8): (8, 4, 4)}[sizes]
    in_specs = (
        P(("fs", "tp"), None),
        P("fs", "tp"),
        P("fs", "tp"),
        P("fs", "tp"),
        P("fs", "tp"),
        P(None, "tp"),
        P("tp"),
        P("fs", "tp"),
    )
    out_specs = (P(("fs", "tp"), None), P("fs", "tp"), P("fs", "tp"), P(None, "tp"), P("tp"))
    return jax.shard_map(
        functools.partial(on_device, dims),
        mesh=mesh,
        in_specs=in_specs,
        out_specs=out_specs,
        check_vma=False,
    )
```

```python
import functools

import jax
import jax.numpy as jnp
from jax import lax
from jax.experimental import pallas as pl
from jax.experimental.pallas import tpu as pltpu
from jax.sharding import PartitionSpec as P

MESH = pl.DeviceIdType.MESH
F32 = jnp.float32
BF16 = jnp.bfloat16
NC = 2
SUB = 16
LANES = 128

ORDER = (
    41, 40, 43, 44, 45, 46, 34, 16, 47, 48, 0, 49, 50, 35, 51, 52, 17, 4, 20, 53,
    38, 22, 8, 18, 60, 24, 1, 26, 36, 21, 12, 128, 23, 133, 19, 123, 129, 130, 9, 27,
    39, 25, 5, 54, 134, 135, 2, 124, 125, 28, 37, 131, 42, 63, 74, 94, 30, 13, 65, 100,
    64, 97, 84, 29, 70, 79, 10, 69, 95, 75, 31, 67, 106, 14, 6, 153, 98, 148, 80, 89,
    101, 66, 154, 76, 96, 118, 103, 112, 132, 107, 155, 85, 68, 109, 32, 149, 150, 81, 136, 99,
    55, 61, 126, 90, 138, 156, 77, 143, 151, 102, 119, 7, 139, 140, 104, 137, 15, 3, 115, 11,
    86, 113, 144, 145, 127, 82, 56, 157, 108, 91, 152, 110, 78, 71, 141, 33, 158, 146, 105, 120,
    159, 160, 87, 142, 116, 83, 57, 147, 114, 92, 161, 111, 121, 88, 72, 58, 162, 93, 117, 73,
    122, 59, 62,
)


class Plan:
    def __init__(self):
        self.messages = {}
        self.arrivals = {}
        self.tasks = {}

    def message(self, name, link, source, target, device, arrival, group):
        self.messages[name] = (link, source, target, device, arrival, group)
        self.arrivals[arrival][1].append(name)

    def arrival(self, name, whole):
        self.arrivals[name] = (whole, [])

    def task(self, name, rank, cost, body=None, waits=(), after=(), sends=()):
        self.tasks[name] = (rank, cost, body, tuple(waits), tuple(after), tuple(sends))

    def order(self):
        names = list(self.tasks)
        listed = [names[i] for i in ORDER]
        assert sorted(listed) == sorted(names)
        sent, done = set(), set()
        for name in listed:
            rank, cost, body, waits, after, sends = self.tasks[name]
            assert all(m in sent for w in waits for m in self.arrivals[w][1]), name
            assert all(a in done for a in after), name
            sent.update(sends)
            done.add(name)
        assert sent == set(self.messages)
        return listed


def nbytes_of(ref):
    size = ref.dtype.itemsize
    for s in ref.shape:
        size *= s
    return size


def kernel(
    dims,
    tokens,
    gate_in,
    value_in,
    wg_in,
    wv_in,
    cw_in,
    cb_in,
    hidden_in,
    ig_out,
    gg_out,
    vg_out,
    cwg_out,
    cbg_out,
    gate,
    value,
    hidden,
    wgs,
    wvs,
    cw,
    cb,
    tok,
    wa,
    wb,
    gt,
    pa,
    pb,
    az_up,
    az_dn,
    ax_up,
    ax_dn,
    bx_up,
    bx_dn,
    bz_up,
    bz_dn,
    igp,
    twin_in,
    y_up,
    y_dn,
    taps,
    coef,
    terms,
    cx,
    cz,
    load_sem,
    send_sem,
    recv_sem,
):
    nz, nx, ny = dims
    fs, tp = lax.axis_index("fs"), lax.axis_index("tp")
    z, x, y, c = fs // nx, fs % nx, tp // NC, tp % NC
    width, rows = gate.shape
    mine = tok.shape[0] // (ny * NC)
    whole = width // LANES * LANES
    rest = width - whole
    ahead = pa.shape[2]
    shard = wgs.shape[0]
    group = nx * shard
    scale = float(rows * nz * nx) ** (-0.5)

    def at_z(d):
        return (((z + d + nz) % nz) * nx + x, tp)

    def at_x(d):
        return (z * nx + (x + d + nx) % nx, tp)

    def at_y(d):
        return (fs, ((y + d + ny) % ny) * NC + c)

    twin = (fs, y * NC + 1 - c)

    loads = {}
    for i, (name, source, target) in enumerate(
        (
            ("wg", wg_in, wgs),
            ("wv", wv_in, wvs),
            ("tok", tokens, tok.at[pl.ds(tp * mine, mine)]),
            ("gate", gate_in, gate),
            ("value", value_in, value),
            ("hidden", hidden_in, hidden),
            ("cw", cw_in, cw),
            ("cb", cb_in, cb),
        )
    ):
        loads[name] = pltpu.make_async_copy(source, target, load_sem.at[i])
        loads[name].start()
    barrier = pltpu.get_barrier_semaphore()
    peers = (at_z(1), at_z(-1), at_x(1), at_x(-1), at_y(1), at_y(-1), twin)
    for peer in peers:
        pl.semaphore_signal(barrier, inc=1, device_id=peer, device_id_type=MESH)

    loads["wg"].wait()
    loads["wv"].wait()
    wa[fs] = wgs[:, :whole]
    wb[fs, :, :whole] = wvs[:, :whole]
    wb[fs, :, whole:] = jnp.concatenate(
        [wvs[:, whole:].astype(F32), wgs[:, whole:].astype(F32)], axis=1
    ).astype(BF16)
    terms[:, width:] = jnp.zeros((4, terms.shape[1] - width, LANES), F32)
    pl.semaphore_wait(barrier, len(peers))

    plan = Plan()

    def ring_at(axis):
        return {
            "z": (nz, z, at_z),
            "x": (nx, x, at_x),
            "y": (ny, y, at_y),
        }[axis]

    def gather(name, axis, block, half, pair, group, rank, extra=None, first=None):
        n, me, to = ring_at(axis)
        far = n // 2

        def idx(d):
            return (me + d + n) % n

        for h in range(1, far + 1):
            up, dn = idx(1 - h), idx(h - 1)
            su, sd = (block(up), block(dn)) if h < far else (half(up, 0), half(dn, 1))
            plan.arrival(f"{name}.{h}", pair if h < far else block(me))
            plan.message(f"{name}.up{h}", axis + "+", su, su, to(1), f"{name}.{h}", group)
            plan.message(f"{name}.dn{h}", axis + "-", sd, sd, to(-1), f"{name}.{h}", group)
        ends = {0: first}
        for h in range(1, far + 1):
            sends = [f"{name}.up{h + 1}", f"{name}.dn{h + 1}"] if h < far else []
            if extra:
                sends += extra(-h) + extra(h) if h < far else extra(h)
            plan.task(f"{name}.{h}", rank, 0.05, waits=[f"{name}.{h}"], sends=sends)
            ends[h] = f"{name}.{h}"
            if h < far:
                ends[-h] = f"{name}.{h}"
        return [f"{name}.up1", f"{name}.dn1"], ends

    def scatter(name, axis, block, half, up_in, dn_in, half_in, pair, group, rank, cost, ready, last):
        n, me, to = ring_at(axis)
        far = n // 2

        def idx(d):
            return (me + d + n) % n

        for j in range(1, far + 1):
            up, dn = idx(j), idx(-j)
            if j == far:
                su, tu = half(up, 0), half_in(up_in, j - 1, 0)
                sd, td = half(dn, 1), half_in(dn_in, j - 1, 1)
            else:
                su, tu, sd, td = block(up), up_in.at[j - 1], block(dn), dn_in.at[j - 1]
            plan.arrival(f"{name}.{j}", pair if j < far else block(me))
            plan.message(f"{name}.up{j}", axis + "+", su, tu, to(1), f"{name}.{j}", group)
            plan.message(f"{name}.dn{j}", axis + "-", sd, td, to(-1), f"{name}.{j}", group)
        plan.task(
            f"{name}.start", rank, 0.02, after=ready(far), sends=[f"{name}.up{far}", f"{name}.dn{far}"]
        )

        def add(j):
            for sign, h, came in ((1, 0, up_in), (-1, 1, dn_in)):
                at = idx(sign * j)
                if j + 1 == far:
                    own, other = half(at, h), half_in(came, j, h)
                else:
                    own, other = block(at), came.at[j]
                own[...] = (own[...].astype(F32) + other[...].astype(F32)).astype(BF16)

        for j in range(far - 1, 0, -1):
            plan.task(
                f"{name}.{j}",
                rank,
                2 * cost,
                functools.partial(add, j),
                waits=[f"{name}.{j + 1}"],
                after=ready(j) + ready(-j),
                sends=[f"{name}.up{j}", f"{name}.dn{j}"],
            )
        own = block(me)

        def end():
            last(own[...].astype(F32) + up_in[0].astype(F32) + dn_in[0].astype(F32))

        plan.task(
            f"{name}.end", rank, cost * 1.5, end, waits=[f"{name}.1"], after=ready(0)
        )

    offsets_z = [0] + [s * h for h in range(1, nz // 2) for s in (-1, 1)] + [nz // 2]

    offsets_x = [0] + [s * h for h in range(1, nx // 2) for s in (-1, 1)] + [nx // 2]
    az_first, az_ends = {}, {}
    for r in offsets_x:
        col = (x + r + nx) % nx
        az_first[r], az_ends[r] = gather(
            f"waz{r}",
            "z",
            lambda i, col=col: wa.at[i * nx + col],
            lambda i, h, col=col: wa.at[i * nx + col, pl.ds(h * shard // 2, shard // 2)],
            wa.at[pl.ds(0, 2)],
            "wa",
            1,
        )
    ax_first, ax_ends = gather(
        "wax",
        "x",
        lambda i: wa.at[z * nx + i],
        lambda i, h: wa.at[z * nx + i, pl.ds(h * shard // 2, shard // 2)],
        wa.at[pl.ds(0, 2)],
        "wa",
        0,
        extra=lambda r: az_first[r],
    )
    for r in offsets_x:
        az_ends[r][0] = ax_ends[r]
    bx_first, bx_ends = {}, {}
    for d in offsets_z:
        bx_first[d], bx_ends[d] = gather(
            f"wbx{d}",
            "x",
            lambda i, d=d: wb.at[((z + d + nz) % nz) * nx + i],
            lambda i, h, d=d: wb.at[((z + d + nz) % nz) * nx + i, pl.ds(h * shard // 2, shard // 2)],
            wb.at[pl.ds(0, 2)],
            "wb",
            2,
        )
    bz_first, bz_ends = gather(
        "wbz",
        "z",
        lambda i: wb.at[i * nx + x],
        lambda i, h: wb.at[i * nx + x, pl.ds(h * shard // 2, shard // 2)],
        wb.at[pl.ds(0, 2)],
        "wb",
        0,
        extra=lambda d: bx_first[d],
    )

    def tok_at(i):
        return tok.at[pl.ds((i * NC + c) * mine, mine)]

    for d in range(-(ny // 2) + 1, ny // 2 + 1):
        block = tok_at((y + d + ny) % ny)
        plan.arrival(f"twin{d}", block)
        plan.message(f"twin{d}", "twin", block, block, twin, f"twin{d}", "tok")
    tok_first, tok_ends = gather(
        "tok",
        "y",
        tok_at,
        lambda i, h: tok.at[pl.ds((i * NC + c) * mine + h * (mine // 2), mine // 2)],
        tok.at[pl.ds(0, 2 * mine)],
        "tok",
        0,
        extra=lambda d: [f"twin{d}"],
    )
    plan.task("tok.own", 0, 0.02, lambda: loads["tok"].wait(), sends=tok_first + ["twin0"])
    plan.task("go", -1, 0.02, sends=ax_first + bz_first + bx_first[0] + az_first[0])
    plan.task(
        "tok.all",
        3,
        0.02,
        waits=[f"twin{d}" for d in range(-(ny // 2) + 1, ny // 2 + 1)],
        after=[t for t in tok_ends.values() if t] + ["tok.own"],
    )

    k0 = 0.7978845608028654
    k1 = k0 * 0.044715

    lane = lax.broadcasted_iota(jnp.int32, (SUB, LANES), 1)

    def shifted(value, by):
        turned = pltpu.roll(value, by % rows, 1)
        if by > 0:
            edge = jnp.where(lane < by, 0.0, turned[:, :LANES])
            return jnp.concatenate([edge, turned[:, LANES:]], axis=1)
        edge = jnp.where(lane >= LANES + by, 0.0, turned[:, rows - LANES :])
        return jnp.concatenate([turned[:, : rows - LANES], edge], axis=1)

    def act_step(i):
        units = pl.ds(pl.multiple_of(i * SUB, SUB), SUB)
        g = gate[units, :].astype(F32)
        one, two = shifted(g, 1), shifted(g, 2)
        w0, w1, w2 = coef[units, 0:1], coef[units, 1:2], coef[units, 2:3]
        conv = coef[units, 3:4] + w0 * two + w1 * one + w2 * g
        square = conv * conv
        t = jnp.tanh(conv * (k0 + k1 * square))
        cdf = 0.5 + 0.5 * t
        slope = cdf + conv * (0.5 - 0.5 * (t * t)) * (k0 + (3.0 * k1) * square)
        hg = hidden[units, :].astype(F32)
        cg = slope * (hg * value[units, :].astype(F32))
        gg = w2 * cg + w1 * shifted(cg, -1) + w0 * shifted(cg, -2)
        for k, term in enumerate((cg * two, cg * one, cg * g, cg)):
            total = term[:, :LANES]
            for j in range(1, rows // LANES):
                total = total + term[:, j * LANES : (j + 1) * LANES]
            terms[k, units, :] = total
        at = jnp.where(i * SUB < whole, i * SUB, i * SUB + width)
        gt[pl.ds(pl.multiple_of(at, SUB), SUB), :] = gg.astype(BF16)
        at = i * SUB + whole
        gt[pl.ds(pl.multiple_of(at, SUB), SUB), :] = (hg * (conv * cdf)).astype(BF16)

    n_act = 11
    per_act = width // SUB // n_act

    def act(k):
        if k == 0:
            for name in ("gate", "value", "hidden", "cw", "cb"):
                loads[name].wait()
            taps[0:3, :width] = cw[...]
            taps[3, :width] = cb[...]
            coef[...] = taps[...].T

        def step(i, carry):
            act_step(k * per_act + i)
            return carry

        lax.fori_loop(0, per_act, step, 0)

    for k in range(n_act):
        plan.task(f"act{k}", 5, 1.2, functools.partial(act, k), after=[f"act{k - 1}"] if k else [])
    acted = f"act{n_act - 1}"

    pad = taps.shape[1]

    def conv_start():
        sums = jnp.concatenate([terms[k].T.sum(axis=0, keepdims=True) for k in range(4)], axis=0)
        cx[x] = jnp.concatenate([sums[:, : pad // 2], sums[:, pad // 2 :]], axis=0)

    def slots_ring(name, axis, slots):
        return gather(
            name,
            axis,
            lambda i: slots.at[i],
            lambda i, h: slots.at[i, :, pl.ds(h * 2 * LANES, (2 - h) * LANES)],
            slots.at[pl.ds(0, 2)],
            name,
            4,
        )

    cx_first, cx_ends = slots_ring("cx", "x", cx)
    cz_first, cz_ends = slots_ring("cz", "z", cz)
    cx_names = [t for t in cx_ends.values() if t]
    cz_names = [t for t in cz_ends.values() if t]

    def conv_middle():
        total = cx[0]
        for i in range(1, nx):
            total = total + cx[i]
        cz[z] = total

    def conv_end():
        total = cz[0]
        for i in range(1, nz):
            total = total + cz[i]
        total = total * scale
        total = jnp.concatenate([total[:4], total[4:]], axis=1)[:, :width]
        cwg_out[...] = total[:3]
        cbg_out[...] = total[3]

    plan.task("conv.start", 6, 0.2, conv_start, after=[acted], sends=cx_first)
    plan.task("conv.middle", 6, 0.1, conv_middle, after=cx_names + ["conv.start"], sends=cz_first)
    plan.task("conv.end", 9, 0.1, conv_end, after=cz_names + ["conv.middle"])

    grad_order = [nz // 2] + [s * h for h in range(nz // 2 - 1, 0, -1) for s in (1, -1)] + [0]

    def grad(d):
        to_z = (z + d + nz) % nz
        left = tok[:, pl.ds(pl.multiple_of(to_z * group, group), group)]
        over_rows = (((0,), (1,)), ((), ()))
        for right, out in ((gt.at[:ahead], pa), (gt.at[ahead:], pb)):
            part = lax.dot_general(left, right[...], over_rows, preferred_element_type=F32)
            out[pl.ds(to_z * nx, nx)] = part.astype(BF16).reshape(nx, shard, part.shape[1])

    for d in grad_order:
        plan.task(f"grad{d}", 7, 1.2, functools.partial(grad, d), after=["tok.all", acted])

    def ax_last(total):
        gg_out[:, :ahead] = total * scale

    def az_last(r, total):
        pa[z * nx + (x + r + nx) % nx] = total.astype(BF16)

    scatter(
        "pax",
        "x",
        lambda i: pa.at[z * nx + i],
        lambda i, h: pa.at[z * nx + i, pl.ds(h * shard // 2, shard // 2)],
        ax_up,
        ax_dn,
        lambda ref, j, h: ref.at[j, pl.ds(h * shard // 2, shard // 2)],
        pa.at[pl.ds(0, 2)],
        "pa",
        3,
        0.1,
        lambda d: [f"paz{d}.end"],
        ax_last,
    )
    for i, r in enumerate([nx // 2] + [s * h for h in range(nx // 2 - 1, 0, -1) for s in (1, -1)] + [0]):
        col = (x + r + nx) % nx
        scatter(
            f"paz{r}",
            "z",
            lambda i, col=col: pa.at[i * nx + col],
            lambda i, h, col=col: pa.at[i * nx + col, pl.ds(h * shard // 2, shard // 2)],
            az_up.at[i],
            az_dn.at[i],
            lambda ref, j, h: ref.at[j, pl.ds(h * shard // 2, shard // 2)],
            pa.at[pl.ds(0, 2)],
            "pa",
            2,
            0.1,
            lambda d: [f"grad{d}"],
            functools.partial(az_last, r),
        )

    def bz_last(total):
        total = total * scale
        start = whole - ahead
        gg_out[:, ahead:whole] = total[:, :start]
        vg_out[...] = total[:, start : start + width]
        gg_out[:, whole:] = total[:, start + width :]

    def bx_last(d, total):
        pb[((z + d + nz) % nz) * nx + x] = total.astype(BF16)

    for i, d in enumerate(grad_order):
        scatter(
            f"pbx{d}",
            "x",
            lambda i, d=d: pb.at[((z + d + nz) % nz) * nx + i],
            lambda i, h, d=d: pb.at[((z + d + nz) % nz) * nx + i, pl.ds(h * shard // 2, shard // 2)],
            bx_up.at[i],
            bx_dn.at[i],
            lambda ref, j, h: ref.at[j, pl.ds(h * shard // 2, shard // 2)],
            pb.at[pl.ds(0, 2)],
            "pb",
            2,
            0.1,
            lambda e, d=d: [f"grad{d}"],
            functools.partial(bx_last, d),
        )
    scatter(
        "pbz",
        "z",
        lambda i: pb.at[i * nx + x],
        lambda i, h: pb.at[i * nx + x, pl.ds(h * shard // 2, shard // 2)],
        bz_up,
        bz_dn,
        lambda ref, j, h: ref.at[j, pl.ds(h * shard // 2, shard // 2)],
        pb.at[pl.ds(0, 2)],
        "pb",
        2,
        0.1,
        lambda d: [f"pbx{d}.end"],
        bz_last,
    )


    def ig(d):
        at = (z + d + nz) % nz
        left_w = wa[pl.ds(at * nx, nx)].reshape(group, whole)
        right_w = wb[pl.ds(at * nx, nx)].reshape(group, 2 * width - whole)
        part = jnp.dot(left_w, gt[:whole], preferred_element_type=F32)
        part = part + jnp.dot(right_w, gt[whole:], preferred_element_type=F32)
        part = part.astype(BF16)
        for k in range(ny * NC):
            igp[at, k % NC, k // NC] = part[:, k * mine : (k + 1) * mine]

    for d in offsets_z:
        at = (z + d + nz) % nz
        m = f"igt{d}"
        source, target = igp.at[at, 1 - c], twin_in.at[at]
        plan.arrival(m, source)
        plan.message(m, "twin", source, target, twin, m, "ig")
        ends = [a[d] for a in az_ends.values()] + [bz_ends[d], *bx_ends[d].values()]
        ends = [t for t in ends if t]
        plan.task(f"ig{d}", 8, 1.1, functools.partial(ig, d), after=[acted] + ends, sends=[m])

        def merge(at=at):
            igp[at, c] = (igp[at, c].astype(F32) + twin_in[at].astype(F32)).astype(BF16)

        plan.task(f"igm{d}", 3, 0.2, merge, waits=[m], after=[f"ig{d}"])

        def ig_last(total, at=at):
            ig_out[:, pl.ds(pl.multiple_of(at * group, group), group)] = total.T.astype(BF16)

        scatter(
            f"igy{d}",
            "y",
            lambda i, at=at: igp.at[at, c, i],
            lambda i, h, at=at: igp.at[at, c, i, pl.ds(h * (group // 2), group // 2)],
            y_up.at[at],
            y_dn.at[at],
            lambda ref, j, h: ref.at[j, pl.ds(h * (group // 2), group // 2)],
            igp.at[0, 0, pl.ds(0, 2)],
            "ig",
            3,
            0.05,
            lambda e, d=d: [f"igm{d}"],
            ig_last,
        )

    left_from = {
        "wa": wa.at[pl.ds(0, nz * nx - 1)],
        "wb": wb.at[pl.ds(0, nz * nx - 1)],
        "tok": tok.at[pl.ds(0, (2 * ny - 1) * mine)],
        "pa": pa.at[pl.ds(0, nz * nx - 1)],
        "pb": pb.at[pl.ds(0, nz * nx - 1)],
        "ig": igp.at[pl.ds(0, nz * (2 * ny - 1) // (NC * ny))],
        "cx": cx.at[pl.ds(0, nx - 1)],
        "cz": cz.at[pl.ds(0, nz - 1)],
    }
    send_at = {name: send_sem.at[i] for i, name in enumerate(left_from)}
    recv_at = {name: recv_sem.at[i] for i, name in enumerate(plan.arrivals)}
    assert len(recv_at) == recv_sem.shape[0] and len(send_at) == send_sem.shape[0]
    for name, whole_ref in left_from.items():
        sizes = [nbytes_of(v[1]) for v in plan.messages.values() if v[5] == name]
        assert sum(sizes) == nbytes_of(whole_ref), name

    def remote(source, target, device, sent, arrival):
        return pltpu.make_async_remote_copy(
            src_ref=source,
            dst_ref=target,
            send_sem=send_at[sent],
            recv_sem=recv_at[arrival],
            device_id=device,
            device_id_type=MESH,
        )

    for name, (whole_ref, names) in plan.arrivals.items():
        assert sum(nbytes_of(plan.messages[m][2]) for m in names) == nbytes_of(whole_ref), name
    for name in plan.order():
        rank, cost, body, waits, after, sends = plan.tasks[name]
        for w in waits:
            ref, names = plan.arrivals[w]
            remote(ref, ref, twin, plan.messages[names[0]][5], w).wait_recv()
        if body is not None:
            body()
        for m in sends:
            remote(*plan.messages[m][1:4], plan.messages[m][5], plan.messages[m][4]).start()
    for name, ref in left_from.items():
        remote(ref, ref, twin, name, next(iter(recv_at))).wait_send()


def put_out(*refs):
    copies = [pltpu.make_async_copy(refs[i], refs[5 + i], refs[10].at[i]) for i in range(5)]
    for copy in copies:
        copy.start()
    for copy in copies:
        copy.wait()


def on_device(dims, *args):
    tokens, gate_pre, value_pre, up_gate_w, up_value_w, conv_weight, conv_bias, hidden_grad = args
    nz, nx, ny = dims
    rows, width = gate_pre.shape
    mine, model = tokens.shape
    shard = up_gate_w.shape[0]
    whole = width // LANES * LANES
    ca, cb = whole, 2 * width - whole
    pa, pb = whole - LANES, 2 * width - whole + LANES
    pad = whole + LANES
    group = nx * shard
    n_arrivals = (3 + 2 * nz) * (nx // 2) + (3 + 2 * nx) * (nz // 2) + (nz + 1) * (ny // 2) + ny + nz
    outs = (
        ((mine, model), BF16),
        ((shard, width), F32),
        ((shard, width), F32),
        ((3, width), F32),
        ((width,), F32),
    )
    results = pl.pallas_call(
        functools.partial(kernel, dims),
        out_shape=[pltpu.VMEM(*out) for out in outs],
        in_specs=[pl.BlockSpec(memory_space=pltpu.HBM)] * 8,
        out_specs=[pl.BlockSpec(memory_space=pltpu.VMEM)] * 5,
        scratch_shapes=[
            pltpu.VMEM((width, rows), BF16),
            pltpu.VMEM((width, rows), BF16),
            pltpu.VMEM((width, rows), BF16),
            pltpu.VMEM((shard, width), BF16),
            pltpu.VMEM((shard, width), BF16),
            pltpu.VMEM((3, width), F32),
            pltpu.VMEM((width,), F32),
            pltpu.VMEM((mine * ny * NC, model), BF16),
            pltpu.VMEM((nz * nx, shard, ca), BF16),
            pltpu.VMEM((nz * nx, shard, cb), BF16),
            pltpu.VMEM((2 * width, rows), BF16),
            pltpu.VMEM((nz * nx, shard, pa), BF16),
            pltpu.VMEM((nz * nx, shard, pb), BF16),
            pltpu.VMEM((nx, nz // 2, shard, pa), BF16),
            pltpu.VMEM((nx, nz // 2, shard, pa), BF16),
            pltpu.VMEM((nx // 2, shard, pa), BF16),
            pltpu.VMEM((nx // 2, shard, pa), BF16),
            pltpu.VMEM((nz, nx // 2, shard, pb), BF16),
            pltpu.VMEM((nz, nx // 2, shard, pb), BF16),
            pltpu.VMEM((nz // 2, shard, pb), BF16),
            pltpu.VMEM((nz // 2, shard, pb), BF16),
            pltpu.VMEM((nz, NC, ny, group, mine), BF16),
            pltpu.VMEM((nz, ny, group, mine), BF16),
            pltpu.VMEM((nz, ny // 2, group, mine), BF16),
            pltpu.VMEM((nz, ny // 2, group, mine), BF16),
            pltpu.VMEM((8, pad), F32),
            pltpu.VMEM((pad, 8), F32),
            pltpu.VMEM((4, pad, LANES), F32),
            pltpu.VMEM((nx, 8, pad // 2), F32),
            pltpu.VMEM((nz, 8, pad // 2), F32),
            pltpu.SemaphoreType.DMA((8,)),
            pltpu.SemaphoreType.DMA((8,)),
            pltpu.SemaphoreType.DMA((n_arrivals,)),
        ],
        compiler_params=pltpu.CompilerParams(
            collective_id=0, has_side_effects=True, vmem_limit_bytes=56_000_000
        ),
    )(
        *(
            pltpu.with_memory_space_constraint(a, pltpu.HBM)
            for a in (
                tokens,
                gate_pre.T,
                value_pre.T,
                up_gate_w,
                up_value_w,
                conv_weight,
                conv_bias,
                hidden_grad.T,
            )
        )
    )
    return pl.pallas_call(
        put_out,
        out_shape=[jax.ShapeDtypeStruct(*out) for out in outs],
        in_specs=[pl.BlockSpec(memory_space=pltpu.VMEM)] * 5,
        out_specs=[pl.BlockSpec(memory_space=pltpu.HBM)] * 5,
        scratch_shapes=[pltpu.SemaphoreType.DMA((5,))],
    )(*(pltpu.with_memory_space_constraint(r, pltpu.VMEM) for r in results))


def solution(mesh):
    sizes = (mesh.shape["fs"], mesh.shape["tp"])
    dims = {(32, 8): (8, 4, 4)}[sizes]
    in_specs = (
        P(("fs", "tp"), None),
        P("fs", "tp"),
        P("fs", "tp"),
        P("fs", "tp"),
        P("fs", "tp"),
        P(None, "tp"),
        P("tp"),
        P("fs", "tp"),
    )
    out_specs = (P(("fs", "tp"), None), P("fs", "tp"), P("fs", "tp"), P(None, "tp"), P("tp"))
    return jax.shard_map(
        functools.partial(on_device, dims),
        mesh=mesh,
        in_specs=in_specs,
        out_specs=out_specs,
        check_vma=False,
    )
```

```python
import functools

import jax
import jax.numpy as jnp
from jax import lax
from jax.experimental import pallas as pl
from jax.experimental.pallas import tpu as pltpu
from jax.sharding import PartitionSpec as P

MESH = pl.DeviceIdType.MESH
F32 = jnp.float32
BF16 = jnp.bfloat16
NC = 2
SUB = 16
LANES = 128

ORDER = (
    41, 40, 43, 44, 45, 46, 34, 16, 47, 48, 0, 49, 50, 20, 35, 51, 52, 22, 17, 53,
    8, 38, 62, 4, 21, 18, 1, 24, 36, 26, 12, 131, 23, 136, 19, 126, 132, 133, 25, 5,
    54, 9, 39, 137, 138, 28, 2, 127, 128, 37, 134, 30, 42, 66, 77, 82, 55, 13, 97, 63,
    87, 68, 103, 29, 6, 70, 109, 67, 100, 27, 72, 78, 98, 83, 69, 104, 106, 3, 14, 71,
    56, 92, 10, 151, 101, 7, 31, 156, 79, 99, 121, 135, 32, 152, 153, 84, 88, 146, 57, 93,
    15, 157, 158, 105, 112, 115, 141, 154, 107, 147, 11, 80, 148, 129, 139, 110, 73, 159, 118, 102,
    142, 143, 122, 85, 33, 161, 155, 113, 58, 89, 149, 116, 130, 94, 162, 163, 140, 81, 74, 108,
    160, 144, 111, 123, 150, 86, 164, 59, 64, 119, 90, 145, 95, 114, 165, 117, 124, 60, 91, 75,
    96, 120, 61, 65, 125, 76,
)


class Plan:
    def __init__(self):
        self.messages = {}
        self.arrivals = {}
        self.tasks = {}

    def message(self, name, link, source, target, device, arrival, group):
        self.messages[name] = (link, source, target, device, arrival, group)
        self.arrivals[arrival][1].append(name)

    def arrival(self, name, whole):
        self.arrivals[name] = (whole, [])

    def task(self, name, rank, cost, body=None, waits=(), after=(), sends=()):
        self.tasks[name] = (rank, cost, body, tuple(waits), tuple(after), tuple(sends))

    def order(self):
        names = list(self.tasks)
        listed = [names[i] for i in ORDER]
        assert sorted(listed) == sorted(names)
        sent, done = set(), set()
        for name in listed:
            rank, cost, body, waits, after, sends = self.tasks[name]
            assert all(m in sent for w in waits for m in self.arrivals[w][1]), name
            assert all(a in done for a in after), name
            sent.update(sends)
            done.add(name)
        assert sent == set(self.messages)
        return listed


def nbytes_of(ref):
    size = ref.dtype.itemsize
    for s in ref.shape:
        size *= s
    return size


def kernel(
    dims,
    tokens,
    gate_in,
    value_in,
    wg_in,
    wv_in,
    cw_in,
    cb_in,
    hidden_in,
    ig_out,
    gg_out,
    vg_out,
    cwg_out,
    cbg_out,
    gate,
    value,
    hidden,
    wgs,
    wvs,
    cw,
    cb,
    tok,
    wa,
    wb,
    gt,
    pa,
    pb,
    az_up,
    az_dn,
    ax_up,
    ax_dn,
    bx_up,
    bx_dn,
    bz_up,
    bz_dn,
    igp,
    twin_in,
    y_up,
    y_dn,
    taps,
    coef,
    terms,
    cx,
    cz,
    ct,
    csum,
    load_sem,
    send_sem,
    recv_sem,
):
    nz, nx, ny = dims
    fs, tp = lax.axis_index("fs"), lax.axis_index("tp")
    z, x, y, c = fs // nx, fs % nx, tp // NC, tp % NC
    width, rows = gate.shape
    mine = tok.shape[0] // (ny * NC)
    whole = width // LANES * LANES
    rest = width - whole
    ahead = pa.shape[2]
    shard = wgs.shape[0]
    group = nx * shard
    scale = float(rows * nz * nx) ** (-0.5)

    def at_z(d):
        return (((z + d + nz) % nz) * nx + x, tp)

    def at_x(d):
        return (z * nx + (x + d + nx) % nx, tp)

    def at_y(d):
        return (fs, ((y + d + ny) % ny) * NC + c)

    twin = (fs, y * NC + 1 - c)

    loads = {}
    for i, (name, source, target) in enumerate(
        (
            ("wg", wg_in, wgs),
            ("wv", wv_in, wvs),
            ("tok", tokens, tok.at[pl.ds(tp * mine, mine)]),
            ("gate", gate_in, gate),
            ("value", value_in, value),
            ("hidden", hidden_in, hidden),
            ("cw", cw_in, cw),
            ("cb", cb_in, cb),
        )
    ):
        loads[name] = pltpu.make_async_copy(source, target, load_sem.at[i])
        loads[name].start()
    barrier = pltpu.get_barrier_semaphore()
    peers = (at_z(1), at_z(-1), at_x(1), at_x(-1), at_y(1), at_y(-1), twin)
    for peer in peers:
        pl.semaphore_signal(barrier, inc=1, device_id=peer, device_id_type=MESH)

    loads["wg"].wait()
    loads["wv"].wait()
    wa[fs] = wgs[:, :whole]
    wb[fs, :, :whole] = wvs[:, :whole]
    wb[fs, :, whole:] = jnp.concatenate(
        [wvs[:, whole:].astype(F32), wgs[:, whole:].astype(F32)], axis=1
    ).astype(BF16)
    terms[:, width:] = jnp.zeros((4, terms.shape[1] - width, LANES), F32)
    pl.semaphore_wait(barrier, len(peers))

    plan = Plan()

    def ring_at(axis):
        return {
            "z": (nz, z, at_z),
            "x": (nx, x, at_x),
            "y": (ny, y, at_y),
        }[axis]

    def gather(name, axis, block, half, pair, group, rank, extra=None, first=None):
        n, me, to = ring_at(axis)
        far = n // 2

        def idx(d):
            return (me + d + n) % n

        for h in range(1, far + 1):
            up, dn = idx(1 - h), idx(h - 1)
            su, sd = (block(up), block(dn)) if h < far else (half(up, 0), half(dn, 1))
            plan.arrival(f"{name}.{h}", pair if h < far else block(me))
            plan.message(f"{name}.up{h}", axis + "+", su, su, to(1), f"{name}.{h}", group)
            if sd is not None:
                plan.message(f"{name}.dn{h}", axis + "-", sd, sd, to(-1), f"{name}.{h}", group)
        ends = {0: first}
        for h in range(1, far + 1):
            sends = [m for m in (f"{name}.up{h + 1}", f"{name}.dn{h + 1}") if m in plan.messages]
            if extra:
                sends += extra(-h) + extra(h) if h < far else extra(h)
            plan.task(f"{name}.{h}", rank, 0.05, waits=[f"{name}.{h}"], sends=sends)
            ends[h] = f"{name}.{h}"
            if h < far:
                ends[-h] = f"{name}.{h}"
        return [f"{name}.up1", f"{name}.dn1"], ends

    def scatter(name, axis, block, half, up_in, dn_in, half_in, pair, group, rank, cost, ready, last):
        n, me, to = ring_at(axis)
        far = n // 2

        def idx(d):
            return (me + d + n) % n

        for j in range(1, far + 1):
            up, dn = idx(j), idx(-j)
            if j == far:
                su, tu = half(up, 0), half_in(up_in, j - 1, 0)
                sd, td = half(dn, 1), half_in(dn_in, j - 1, 1)
            else:
                su, tu, sd, td = block(up), up_in.at[j - 1], block(dn), dn_in.at[j - 1]
            plan.arrival(f"{name}.{j}", pair if j < far else block(me))
            plan.message(f"{name}.up{j}", axis + "+", su, tu, to(1), f"{name}.{j}", group)
            plan.message(f"{name}.dn{j}", axis + "-", sd, td, to(-1), f"{name}.{j}", group)
        plan.task(
            f"{name}.start", rank, 0.02, after=ready(far), sends=[f"{name}.up{far}", f"{name}.dn{far}"]
        )

        def add(j):
            for sign, h, came in ((1, 0, up_in), (-1, 1, dn_in)):
                at = idx(sign * j)
                if j + 1 == far:
                    own, other = half(at, h), half_in(came, j, h)
                else:
                    own, other = block(at), came.at[j]
                own[...] = (own[...].astype(F32) + other[...].astype(F32)).astype(BF16)

        for j in range(far - 1, 0, -1):
            plan.task(
                f"{name}.{j}",
                rank,
                2 * cost,
                functools.partial(add, j),
                waits=[f"{name}.{j + 1}"],
                after=ready(j) + ready(-j),
                sends=[f"{name}.up{j}", f"{name}.dn{j}"],
            )
        own = block(me)

        def end():
            last(own[...].astype(F32) + up_in[0].astype(F32) + dn_in[0].astype(F32))

        plan.task(
            f"{name}.end", rank, cost * 1.5, end, waits=[f"{name}.1"], after=ready(0)
        )

    offsets_z = [0] + [s * h for h in range(1, nz // 2) for s in (-1, 1)] + [nz // 2]

    offsets_x = [0] + [s * h for h in range(1, nx // 2) for s in (-1, 1)] + [nx // 2]
    az_first, az_ends = {}, {}
    for r in offsets_x:
        col = (x + r + nx) % nx
        az_first[r], az_ends[r] = gather(
            f"waz{r}",
            "z",
            lambda i, col=col: wa.at[i * nx + col],
            lambda i, h, col=col: wa.at[i * nx + col, pl.ds(h * shard // 2, shard // 2)],
            wa.at[pl.ds(0, 2)],
            "wa",
            1,
        )
    ax_first, ax_ends = gather(
        "wax",
        "x",
        lambda i: wa.at[z * nx + i],
        lambda i, h: wa.at[z * nx + i, pl.ds(h * shard // 2, shard // 2)],
        wa.at[pl.ds(0, 2)],
        "wa",
        0,
        extra=lambda r: az_first[r],
    )
    for r in offsets_x:
        az_ends[r][0] = ax_ends[r]
    bx_first, bx_ends = {}, {}
    for d in offsets_z:
        bx_first[d], bx_ends[d] = gather(
            f"wbx{d}",
            "x",
            lambda i, d=d: wb.at[((z + d + nz) % nz) * nx + i],
            lambda i, h, d=d: wb.at[((z + d + nz) % nz) * nx + i, pl.ds(h * shard // 2, shard // 2)],
            wb.at[pl.ds(0, 2)],
            "wb",
            2,
        )
    bz_first, bz_ends = gather(
        "wbz",
        "z",
        lambda i: wb.at[i * nx + x],
        lambda i, h: wb.at[i * nx + x, pl.ds(h * shard // 2, shard // 2)],
        wb.at[pl.ds(0, 2)],
        "wb",
        0,
        extra=lambda d: bx_first[d],
    )

    def tok_at(i):
        return tok.at[pl.ds((i * NC + c) * mine, mine)]

    for d in range(-(ny // 2) + 1, ny // 2 + 1):
        block = tok_at((y + d + ny) % ny)
        plan.arrival(f"twin{d}", block)
        plan.message(f"twin{d}", "twin", block, block, twin, f"twin{d}", "tok")
    tok_first, tok_ends = gather(
        "tok",
        "y",
        tok_at,
        lambda i, h: tok.at[pl.ds((i * NC + c) * mine + h * (mine // 2), mine // 2)],
        tok.at[pl.ds(0, 2 * mine)],
        "tok",
        0,
        extra=lambda d: [f"twin{d}"],
    )
    plan.task("tok.own", 0, 0.02, lambda: loads["tok"].wait(), sends=tok_first + ["twin0"])
    plan.task("go", -1, 0.02, sends=ax_first + bz_first + bx_first[0] + az_first[0])
    plan.task(
        "tok.all",
        3,
        0.02,
        waits=[f"twin{d}" for d in range(-(ny // 2) + 1, ny // 2 + 1)],
        after=[t for t in tok_ends.values() if t] + ["tok.own"],
    )

    k0 = 0.7978845608028654
    k1 = k0 * 0.044715

    lane = lax.broadcasted_iota(jnp.int32, (SUB, LANES), 1)

    def shifted(value, by):
        turned = pltpu.roll(value, by % rows, 1)
        if by > 0:
            edge = jnp.where(lane < by, 0.0, turned[:, :LANES])
            return jnp.concatenate([edge, turned[:, LANES:]], axis=1)
        edge = jnp.where(lane >= LANES + by, 0.0, turned[:, rows - LANES :])
        return jnp.concatenate([turned[:, : rows - LANES], edge], axis=1)

    def act_step(i):
        units = pl.ds(pl.multiple_of(i * SUB, SUB), SUB)
        g = gate[units, :].astype(F32)
        one, two = shifted(g, 1), shifted(g, 2)
        w0, w1, w2 = coef[units, 0:1], coef[units, 1:2], coef[units, 2:3]
        conv = coef[units, 3:4] + w0 * two + w1 * one + w2 * g
        square = conv * conv
        t = jnp.tanh(conv * (k0 + k1 * square))
        cdf = 0.5 + 0.5 * t
        slope = cdf + conv * (0.5 - 0.5 * (t * t)) * (k0 + (3.0 * k1) * square)
        hg = hidden[units, :].astype(F32)
        cg = slope * (hg * value[units, :].astype(F32))
        gg = w2 * cg + w1 * shifted(cg, -1) + w0 * shifted(cg, -2)
        for k, term in enumerate((cg * two, cg * one, cg * g, cg)):
            total = term[:, :LANES]
            for j in range(1, rows // LANES):
                total = total + term[:, j * LANES : (j + 1) * LANES]
            terms[k, units, :] = total
        at = jnp.where(i * SUB < whole, i * SUB, i * SUB + width)
        gt[pl.ds(pl.multiple_of(at, SUB), SUB), :] = gg.astype(BF16)
        at = i * SUB + whole
        gt[pl.ds(pl.multiple_of(at, SUB), SUB), :] = (hg * (conv * cdf)).astype(BF16)

    n_act = 11
    per_act = width // SUB // n_act

    def act(k):
        if k == 0:
            for name in ("gate", "value", "hidden", "cw", "cb"):
                loads[name].wait()
            taps[0:3, :width] = cw[...]
            taps[3, :width] = cb[...]
            coef[...] = taps[...].T

        def step(i, carry):
            act_step(k * per_act + i)
            return carry

        lax.fori_loop(0, per_act, step, 0)

    for k in range(n_act):
        plan.task(f"act{k}", 5, 1.2, functools.partial(act, k), after=[f"act{k - 1}"] if k else [])
    acted = f"act{n_act - 1}"

    pad = taps.shape[1]

    def conv_start():
        sums = jnp.concatenate([terms[k].T.sum(axis=0, keepdims=True) for k in range(4)], axis=0)
        cx[x] = jnp.concatenate([sums[:, : pad // 2], sums[:, pad // 2 :]], axis=0)

    def slots_ring(name, axis, slots):
        pair = slots.at[pl.ds(0, 2)]
        first, ends = gather(
            name, axis, lambda i: slots.at[i], lambda i, h: None if h else slots.at[i], pair, name, 4
        )
        return first, [t for t in ends.values() if t]

    cx_first, cx_names = slots_ring("cx", "x", cx)
    cz_first, cz_names = slots_ring("cz", "z", cz)
    ct_first, ct_names = slots_ring("ct", "x", ct)
    tiles = pad // 2 // LANES

    def total_of(slots, n):
        total = slots[0]
        for i in range(1, n):
            total = total + slots[i]
        return total

    def conv_middle():
        total = total_of(cx, nx)
        for j in range(tiles):
            csum[j] = total[:, j * LANES : (j + 1) * LANES]
        cz[z] = csum[jnp.minimum(x, tiles - 1)]

    def conv_late():
        ct[x] = total_of(cz, nz)

    def conv_end():
        total = jnp.concatenate([ct[j] for j in range(tiles)], axis=1) * scale
        total = jnp.concatenate([total[:4], total[4:]], axis=1)[:, :width]
        cwg_out[...] = total[:3]
        cbg_out[...] = total[3]

    plan.task("conv.start", 6, 0.2, conv_start, after=[acted], sends=cx_first)
    plan.task("conv.middle", 6, 0.1, conv_middle, after=cx_names + ["conv.start"], sends=cz_first)
    plan.task("conv.late", 6, 0.1, conv_late, after=cz_names + ["conv.middle"], sends=ct_first)
    plan.task("conv.end", 9, 0.1, conv_end, after=ct_names + ["conv.late"])

    grad_order = [nz // 2] + [s * h for h in range(nz // 2 - 1, 0, -1) for s in (1, -1)] + [0]

    def grad(d):
        to_z = (z + d + nz) % nz
        left = tok[:, pl.ds(pl.multiple_of(to_z * group, group), group)]
        over_rows = (((0,), (1,)), ((), ()))
        for right, out in ((gt.at[:ahead], pa), (gt.at[ahead:], pb)):
            part = lax.dot_general(left, right[...], over_rows, preferred_element_type=F32)
            out[pl.ds(to_z * nx, nx)] = part.astype(BF16).reshape(nx, shard, part.shape[1])

    for d in grad_order:
        plan.task(f"grad{d}", 7, 1.2, functools.partial(grad, d), after=["tok.all", acted])

    def ax_last(total):
        gg_out[:, :ahead] = total * scale

    def az_last(r, total):
        pa[z * nx + (x + r + nx) % nx] = total.astype(BF16)

    scatter(
        "pax",
        "x",
        lambda i: pa.at[z * nx + i],
        lambda i, h: pa.at[z * nx + i, pl.ds(h * shard // 2, shard // 2)],
        ax_up,
        ax_dn,
        lambda ref, j, h: ref.at[j, pl.ds(h * shard // 2, shard // 2)],
        pa.at[pl.ds(0, 2)],
        "pa",
        3,
        0.1,
        lambda d: [f"paz{d}.end"],
        ax_last,
    )
    for i, r in enumerate([nx // 2] + [s * h for h in range(nx // 2 - 1, 0, -1) for s in (1, -1)] + [0]):
        col = (x + r + nx) % nx
        scatter(
            f"paz{r}",
            "z",
            lambda i, col=col: pa.at[i * nx + col],
            lambda i, h, col=col: pa.at[i * nx + col, pl.ds(h * shard // 2, shard // 2)],
            az_up.at[i],
            az_dn.at[i],
            lambda ref, j, h: ref.at[j, pl.ds(h * shard // 2, shard // 2)],
            pa.at[pl.ds(0, 2)],
            "pa",
            2,
            0.1,
            lambda d: [f"grad{d}"],
            functools.partial(az_last, r),
        )

    def bz_last(total):
        total = total * scale
        start = whole - ahead
        gg_out[:, ahead:whole] = total[:, :start]
        vg_out[...] = total[:, start : start + width]
        gg_out[:, whole:] = total[:, start + width :]

    def bx_last(d, total):
        pb[((z + d + nz) % nz) * nx + x] = total.astype(BF16)

    for i, d in enumerate(grad_order):
        scatter(
            f"pbx{d}",
            "x",
            lambda i, d=d: pb.at[((z + d + nz) % nz) * nx + i],
            lambda i, h, d=d: pb.at[((z + d + nz) % nz) * nx + i, pl.ds(h * shard // 2, shard // 2)],
            bx_up.at[i],
            bx_dn.at[i],
            lambda ref, j, h: ref.at[j, pl.ds(h * shard // 2, shard // 2)],
            pb.at[pl.ds(0, 2)],
            "pb",
            2,
            0.1,
            lambda e, d=d: [f"grad{d}"],
            functools.partial(bx_last, d),
        )
    scatter(
        "pbz",
        "z",
        lambda i: pb.at[i * nx + x],
        lambda i, h: pb.at[i * nx + x, pl.ds(h * shard // 2, shard // 2)],
        bz_up,
        bz_dn,
        lambda ref, j, h: ref.at[j, pl.ds(h * shard // 2, shard // 2)],
        pb.at[pl.ds(0, 2)],
        "pb",
        2,
        0.1,
        lambda d: [f"pbx{d}.end"],
        bz_last,
    )


    def ig(d):
        at = (z + d + nz) % nz
        left_w = wa[pl.ds(at * nx, nx)].reshape(group, whole)
        right_w = wb[pl.ds(at * nx, nx)].reshape(group, 2 * width - whole)
        part = jnp.dot(left_w, gt[:whole], preferred_element_type=F32)
        part = part + jnp.dot(right_w, gt[whole:], preferred_element_type=F32)
        part = part.astype(BF16)
        for k in range(ny * NC):
            igp[at, k % NC, k // NC] = part[:, k * mine : (k + 1) * mine]

    for d in offsets_z:
        at = (z + d + nz) % nz
        m = f"igt{d}"
        source, target = igp.at[at, 1 - c], twin_in.at[at]
        plan.arrival(m, source)
        plan.message(m, "twin", source, target, twin, m, "ig")
        ends = [a[d] for a in az_ends.values()] + [bz_ends[d], *bx_ends[d].values()]
        ends = [t for t in ends if t]
        plan.task(f"ig{d}", 8, 1.1, functools.partial(ig, d), after=[acted] + ends, sends=[m])

        def merge(at=at):
            igp[at, c] = (igp[at, c].astype(F32) + twin_in[at].astype(F32)).astype(BF16)

        plan.task(f"igm{d}", 3, 0.2, merge, waits=[m], after=[f"ig{d}"])

        def ig_last(total, at=at):
            ig_out[:, pl.ds(pl.multiple_of(at * group, group), group)] = total.T.astype(BF16)

        scatter(
            f"igy{d}",
            "y",
            lambda i, at=at: igp.at[at, c, i],
            lambda i, h, at=at: igp.at[at, c, i, pl.ds(h * (group // 2), group // 2)],
            y_up.at[at],
            y_dn.at[at],
            lambda ref, j, h: ref.at[j, pl.ds(h * (group // 2), group // 2)],
            igp.at[0, 0, pl.ds(0, 2)],
            "ig",
            3,
            0.05,
            lambda e, d=d: [f"igm{d}"],
            ig_last,
        )

    left_from = {
        "wa": wa.at[pl.ds(0, nz * nx - 1)],
        "wb": wb.at[pl.ds(0, nz * nx - 1)],
        "tok": tok.at[pl.ds(0, (2 * ny - 1) * mine)],
        "pa": pa.at[pl.ds(0, nz * nx - 1)],
        "pb": pb.at[pl.ds(0, nz * nx - 1)],
        "ig": igp.at[pl.ds(0, nz * (2 * ny - 1) // (NC * ny))],
        "cx": cx.at[pl.ds(0, nx - 1)],
        "cz": cz.at[pl.ds(0, nz - 1)],
        "ct": ct.at[pl.ds(0, nx - 1)],
    }
    send_at = {name: send_sem.at[i] for i, name in enumerate(left_from)}
    recv_at = {name: recv_sem.at[i] for i, name in enumerate(plan.arrivals)}
    assert len(recv_at) == recv_sem.shape[0] and len(send_at) == send_sem.shape[0]
    for name, whole_ref in left_from.items():
        sizes = [nbytes_of(v[1]) for v in plan.messages.values() if v[5] == name]
        assert sum(sizes) == nbytes_of(whole_ref), name

    def remote(source, target, device, sent, arrival):
        return pltpu.make_async_remote_copy(
            src_ref=source,
            dst_ref=target,
            send_sem=send_at[sent],
            recv_sem=recv_at[arrival],
            device_id=device,
            device_id_type=MESH,
        )

    for name, (whole_ref, names) in plan.arrivals.items():
        assert sum(nbytes_of(plan.messages[m][2]) for m in names) == nbytes_of(whole_ref), name
    for name in plan.order():
        rank, cost, body, waits, after, sends = plan.tasks[name]
        for w in waits:
            ref, names = plan.arrivals[w]
            remote(ref, ref, twin, plan.messages[names[0]][5], w).wait_recv()
        if body is not None:
            body()
        for m in sends:
            remote(*plan.messages[m][1:4], plan.messages[m][5], plan.messages[m][4]).start()
    for name, ref in left_from.items():
        remote(ref, ref, twin, name, next(iter(recv_at))).wait_send()


def put_out(*refs):
    copies = [pltpu.make_async_copy(refs[i], refs[5 + i], refs[10].at[i]) for i in range(5)]
    for copy in copies:
        copy.start()
    for copy in copies:
        copy.wait()


def on_device(dims, *args):
    tokens, gate_pre, value_pre, up_gate_w, up_value_w, conv_weight, conv_bias, hidden_grad = args
    nz, nx, ny = dims
    rows, width = gate_pre.shape
    mine, model = tokens.shape
    shard = up_gate_w.shape[0]
    whole = width // LANES * LANES
    ca, cb = whole, 2 * width - whole
    pa, pb = whole - LANES, 2 * width - whole + LANES
    pad = whole + LANES
    group = nx * shard
    n_arrivals = (4 + 2 * nz) * (nx // 2) + (3 + 2 * nx) * (nz // 2) + (nz + 1) * (ny // 2) + ny + nz
    outs = (
        ((mine, model), BF16),
        ((shard, width), F32),
        ((shard, width), F32),
        ((3, width), F32),
        ((width,), F32),
    )
    results = pl.pallas_call(
        functools.partial(kernel, dims),
        out_shape=[pltpu.VMEM(*out) for out in outs],
        in_specs=[pl.BlockSpec(memory_space=pltpu.HBM)] * 8,
        out_specs=[pl.BlockSpec(memory_space=pltpu.VMEM)] * 5,
        scratch_shapes=[
            pltpu.VMEM((width, rows), BF16),
            pltpu.VMEM((width, rows), BF16),
            pltpu.VMEM((width, rows), BF16),
            pltpu.VMEM((shard, width), BF16),
            pltpu.VMEM((shard, width), BF16),
            pltpu.VMEM((3, width), F32),
            pltpu.VMEM((width,), F32),
            pltpu.VMEM((mine * ny * NC, model), BF16),
            pltpu.VMEM((nz * nx, shard, ca), BF16),
            pltpu.VMEM((nz * nx, shard, cb), BF16),
            pltpu.VMEM((2 * width, rows), BF16),
            pltpu.VMEM((nz * nx, shard, pa), BF16),
            pltpu.VMEM((nz * nx, shard, pb), BF16),
            pltpu.VMEM((nx, nz // 2, shard, pa), BF16),
            pltpu.VMEM((nx, nz // 2, shard, pa), BF16),
            pltpu.VMEM((nx // 2, shard, pa), BF16),
            pltpu.VMEM((nx // 2, shard, pa), BF16),
            pltpu.VMEM((nz, nx // 2, shard, pb), BF16),
            pltpu.VMEM((nz, nx // 2, shard, pb), BF16),
            pltpu.VMEM((nz // 2, shard, pb), BF16),
            pltpu.VMEM((nz // 2, shard, pb), BF16),
            pltpu.VMEM((nz, NC, ny, group, mine), BF16),
            pltpu.VMEM((nz, ny, group, mine), BF16),
            pltpu.VMEM((nz, ny // 2, group, mine), BF16),
            pltpu.VMEM((nz, ny // 2, group, mine), BF16),
            pltpu.VMEM((8, pad), F32),
            pltpu.VMEM((pad, 8), F32),
            pltpu.VMEM((4, pad, LANES), F32),
            pltpu.VMEM((nx, 8, pad // 2), F32),
            pltpu.VMEM((nz, 8, LANES), F32),
            pltpu.VMEM((nx, 8, LANES), F32),
            pltpu.VMEM((pad // 2 // LANES, 8, LANES), F32),
            pltpu.SemaphoreType.DMA((8,)),
            pltpu.SemaphoreType.DMA((9,)),
            pltpu.SemaphoreType.DMA((n_arrivals,)),
        ],
        compiler_params=pltpu.CompilerParams(
            collective_id=0, has_side_effects=True, vmem_limit_bytes=56_000_000
        ),
    )(
        *(
            pltpu.with_memory_space_constraint(a, pltpu.HBM)
            for a in (
                tokens,
                gate_pre.T,
                value_pre.T,
                up_gate_w,
                up_value_w,
                conv_weight,
                conv_bias,
                hidden_grad.T,
            )
        )
    )
    return pl.pallas_call(
        put_out,
        out_shape=[jax.ShapeDtypeStruct(*out) for out in outs],
        in_specs=[pl.BlockSpec(memory_space=pltpu.VMEM)] * 5,
        out_specs=[pl.BlockSpec(memory_space=pltpu.HBM)] * 5,
        scratch_shapes=[pltpu.SemaphoreType.DMA((5,))],
    )(*(pltpu.with_memory_space_constraint(r, pltpu.VMEM) for r in results))


def solution(mesh):
    sizes = (mesh.shape["fs"], mesh.shape["tp"])
    dims = {(32, 8): (8, 4, 4)}[sizes]
    in_specs = (
        P(("fs", "tp"), None),
        P("fs", "tp"),
        P("fs", "tp"),
        P("fs", "tp"),
        P("fs", "tp"),
        P(None, "tp"),
        P("tp"),
        P("fs", "tp"),
    )
    out_specs = (P(("fs", "tp"), None), P("fs", "tp"), P("fs", "tp"), P(None, "tp"), P("tp"))
    return jax.shard_map(
        functools.partial(on_device, dims),
        mesh=mesh,
        in_specs=in_specs,
        out_specs=out_specs,
        check_vma=False,
    )
```

```python
import functools

import jax
import jax.numpy as jnp
from jax import lax
from jax.experimental import pallas as pl
from jax.experimental.pallas import tpu as pltpu
from jax.sharding import PartitionSpec as P

MESH = pl.DeviceIdType.MESH
F32 = jnp.float32
BF16 = jnp.bfloat16
NC = 2
SUB = 16
LANES = 128

ORDER = (
    41, 40, 43, 44, 45, 46, 34, 16, 47, 48, 0, 49, 50, 20, 35, 51, 52, 22, 17, 53,
    8, 38, 62, 4, 21, 18, 1, 24, 36, 26, 12, 131, 23, 136, 19, 126, 132, 133, 25, 5,
    54, 9, 39, 137, 138, 28, 2, 127, 128, 37, 134, 30, 42, 66, 77, 82, 55, 13, 97, 63,
    87, 68, 103, 29, 6, 70, 109, 67, 100, 27, 72, 78, 98, 83, 69, 104, 106, 3, 14, 71,
    56, 92, 10, 151, 101, 7, 31, 156, 79, 99, 121, 135, 32, 152, 153, 84, 88, 146, 57, 93,
    15, 157, 158, 105, 112, 115, 141, 154, 107, 147, 11, 80, 148, 129, 139, 110, 73, 159, 118, 102,
    142, 143, 122, 85, 33, 161, 155, 113, 58, 89, 149, 116, 130, 94, 162, 163, 140, 81, 74, 108,
    160, 144, 111, 123, 150, 86, 164, 59, 64, 119, 90, 145, 95, 114, 165, 117, 124, 60, 91, 75,
    96, 120, 61, 65, 125, 76,
)


class Plan:
    def __init__(self):
        self.messages = {}
        self.arrivals = {}
        self.tasks = {}

    def message(self, name, link, source, target, device, arrival, group):
        self.messages[name] = (link, source, target, device, arrival, group)
        self.arrivals[arrival][1].append(name)

    def arrival(self, name, whole):
        self.arrivals[name] = (whole, [])

    def task(self, name, rank, cost, body=None, waits=(), after=(), sends=()):
        self.tasks[name] = (rank, cost, body, tuple(waits), tuple(after), tuple(sends))

    def order(self):
        names = list(self.tasks)
        listed = [names[i] for i in ORDER]
        assert sorted(listed) == sorted(names)
        sent, done = set(), set()
        for name in listed:
            rank, cost, body, waits, after, sends = self.tasks[name]
            assert all(m in sent for w in waits for m in self.arrivals[w][1]), name
            assert all(a in done for a in after), name
            sent.update(sends)
            done.add(name)
        assert sent == set(self.messages)
        return listed


def nbytes_of(ref):
    size = ref.dtype.itemsize
    for s in ref.shape:
        size *= s
    return size


def kernel(
    dims,
    tokens,
    gate_in,
    value_in,
    wg_in,
    wv_in,
    cw_in,
    cb_in,
    hidden_in,
    ig_out,
    gg_out,
    vg_out,
    cwg_out,
    cbg_out,
    gate,
    value,
    hidden,
    wgs,
    wvs,
    cw,
    cb,
    tok,
    wa,
    wb,
    gt,
    pa,
    pb,
    az_up,
    az_dn,
    ax_up,
    ax_dn,
    bx_up,
    bx_dn,
    bz_up,
    bz_dn,
    igp,
    twin_in,
    y_up,
    y_dn,
    taps,
    coef,
    terms,
    cx,
    cz,
    ct,
    csum,
    load_sem,
    send_sem,
    recv_sem,
):
    nz, nx, ny = dims
    fs, tp = lax.axis_index("fs"), lax.axis_index("tp")
    z, x, y, c = fs // nx, fs % nx, tp // NC, tp % NC
    width, rows = gate.shape
    mine = tok.shape[0] // (ny * NC)
    whole = width // LANES * LANES
    rest = width - whole
    ahead = pa.shape[2]
    shard = wgs.shape[0]
    group = nx * shard
    scale = float(rows * nz * nx) ** (-0.5)

    def at_z(d):
        return (((z + d + nz) % nz) * nx + x, tp)

    def at_x(d):
        return (z * nx + (x + d + nx) % nx, tp)

    def at_y(d):
        return (fs, ((y + d + ny) % ny) * NC + c)

    twin = (fs, y * NC + 1 - c)

    barrier = pltpu.get_barrier_semaphore()
    peers = (at_z(1), at_z(-1), at_x(1), at_x(-1), at_y(1), at_y(-1), twin)
    for peer in peers:
        pl.semaphore_signal(barrier, inc=1, device_id=peer, device_id_type=MESH)
    loads = {}
    for i, (name, source, target) in enumerate(
        (
            ("wg", wg_in, wgs),
            ("wv", wv_in, wvs),
            ("tok", tokens, tok.at[pl.ds(tp * mine, mine)]),
            ("gate", gate_in, gate),
            ("value", value_in, value),
            ("hidden", hidden_in, hidden),
            ("cw", cw_in, cw),
            ("cb", cb_in, cb),
        )
    ):
        loads[name] = pltpu.make_async_copy(source, target, load_sem.at[i])
        loads[name].start()

    loads["wg"].wait()
    loads["wv"].wait()
    wa[fs] = wgs[:, :whole]
    wb[fs, :, :whole] = wvs[:, :whole]
    wb[fs, :, whole:] = jnp.concatenate(
        [wvs[:, whole:].astype(F32), wgs[:, whole:].astype(F32)], axis=1
    ).astype(BF16)
    terms[:, width:] = jnp.zeros((4, terms.shape[1] - width, LANES), F32)
    pl.semaphore_wait(barrier, len(peers))

    plan = Plan()

    def ring_at(axis):
        return {
            "z": (nz, z, at_z),
            "x": (nx, x, at_x),
            "y": (ny, y, at_y),
        }[axis]

    def gather(name, axis, block, half, pair, group, rank, extra=None, first=None):
        n, me, to = ring_at(axis)
        far = n // 2

        def idx(d):
            return (me + d + n) % n

        for h in range(1, far + 1):
            up, dn = idx(1 - h), idx(h - 1)
            su, sd = (block(up), block(dn)) if h < far else (half(up, 0), half(dn, 1))
            plan.arrival(f"{name}.{h}", pair if h < far else block(me))
            plan.message(f"{name}.up{h}", axis + "+", su, su, to(1), f"{name}.{h}", group)
            if sd is not None:
                plan.message(f"{name}.dn{h}", axis + "-", sd, sd, to(-1), f"{name}.{h}", group)
        ends = {0: first}
        for h in range(1, far + 1):
            sends = [m for m in (f"{name}.up{h + 1}", f"{name}.dn{h + 1}") if m in plan.messages]
            if extra:
                sends += extra(-h) + extra(h) if h < far else extra(h)
            plan.task(f"{name}.{h}", rank, 0.05, waits=[f"{name}.{h}"], sends=sends)
            ends[h] = f"{name}.{h}"
            if h < far:
                ends[-h] = f"{name}.{h}"
        return [f"{name}.up1", f"{name}.dn1"], ends

    def scatter(name, axis, block, half, up_in, dn_in, half_in, pair, group, rank, cost, ready, last):
        n, me, to = ring_at(axis)
        far = n // 2

        def idx(d):
            return (me + d + n) % n

        for j in range(1, far + 1):
            up, dn = idx(j), idx(-j)
            if j == far:
                su, tu = half(up, 0), half_in(up_in, j - 1, 0)
                sd, td = half(dn, 1), half_in(dn_in, j - 1, 1)
            else:
                su, tu, sd, td = block(up), up_in.at[j - 1], block(dn), dn_in.at[j - 1]
            plan.arrival(f"{name}.{j}", pair if j < far else block(me))
            plan.message(f"{name}.up{j}", axis + "+", su, tu, to(1), f"{name}.{j}", group)
            plan.message(f"{name}.dn{j}", axis + "-", sd, td, to(-1), f"{name}.{j}", group)
        plan.task(
            f"{name}.start", rank, 0.02, after=ready(far), sends=[f"{name}.up{far}", f"{name}.dn{far}"]
        )

        def add(j, start):
            for way, sign, h, came in (("up", 1, 0, up_in), ("dn", -1, 1, dn_in)):
                at = idx(sign * j)
                if j + 1 == far:
                    own, other = half(at, h), half_in(came, j, h)
                else:
                    own, other = block(at), came.at[j]
                own[...] = (own[...].astype(F32) + other[...].astype(F32)).astype(BF16)
                start(f"{name}.{way}{j}")

        for j in range(far - 1, 0, -1):
            plan.task(
                f"{name}.{j}",
                rank,
                2 * cost,
                (functools.partial(add, j),),
                waits=[f"{name}.{j + 1}"],
                after=ready(j) + ready(-j),
                sends=[f"{name}.up{j}", f"{name}.dn{j}"],
            )
        own = block(me)

        def end():
            last(own[...].astype(F32) + up_in[0].astype(F32) + dn_in[0].astype(F32))

        plan.task(
            f"{name}.end", rank, cost * 1.5, end, waits=[f"{name}.1"], after=ready(0)
        )

    offsets_z = [0] + [s * h for h in range(1, nz // 2) for s in (-1, 1)] + [nz // 2]

    offsets_x = [0] + [s * h for h in range(1, nx // 2) for s in (-1, 1)] + [nx // 2]
    az_first, az_ends = {}, {}
    for r in offsets_x:
        col = (x + r + nx) % nx
        az_first[r], az_ends[r] = gather(
            f"waz{r}",
            "z",
            lambda i, col=col: wa.at[i * nx + col],
            lambda i, h, col=col: wa.at[i * nx + col, pl.ds(h * shard // 2, shard // 2)],
            wa.at[pl.ds(0, 2)],
            "wa",
            1,
        )
    ax_first, ax_ends = gather(
        "wax",
        "x",
        lambda i: wa.at[z * nx + i],
        lambda i, h: wa.at[z * nx + i, pl.ds(h * shard // 2, shard // 2)],
        wa.at[pl.ds(0, 2)],
        "wa",
        0,
        extra=lambda r: az_first[r],
    )
    for r in offsets_x:
        az_ends[r][0] = ax_ends[r]
    bx_first, bx_ends = {}, {}
    for d in offsets_z:
        bx_first[d], bx_ends[d] = gather(
            f"wbx{d}",
            "x",
            lambda i, d=d: wb.at[((z + d + nz) % nz) * nx + i],
            lambda i, h, d=d: wb.at[((z + d + nz) % nz) * nx + i, pl.ds(h * shard // 2, shard // 2)],
            wb.at[pl.ds(0, 2)],
            "wb",
            2,
        )
    bz_first, bz_ends = gather(
        "wbz",
        "z",
        lambda i: wb.at[i * nx + x],
        lambda i, h: wb.at[i * nx + x, pl.ds(h * shard // 2, shard // 2)],
        wb.at[pl.ds(0, 2)],
        "wb",
        0,
        extra=lambda d: bx_first[d],
    )

    def tok_at(i):
        return tok.at[pl.ds((i * NC + c) * mine, mine)]

    for d in range(-(ny // 2) + 1, ny // 2 + 1):
        block = tok_at((y + d + ny) % ny)
        plan.arrival(f"twin{d}", block)
        plan.message(f"twin{d}", "twin", block, block, twin, f"twin{d}", "tok")
    tok_first, tok_ends = gather(
        "tok",
        "y",
        tok_at,
        lambda i, h: tok.at[pl.ds((i * NC + c) * mine + h * (mine // 2), mine // 2)],
        tok.at[pl.ds(0, 2 * mine)],
        "tok",
        0,
        extra=lambda d: [f"twin{d}"],
    )
    plan.task("tok.own", 0, 0.02, lambda: loads["tok"].wait(), sends=tok_first + ["twin0"])
    plan.task("go", -1, 0.02, sends=ax_first + bz_first + bx_first[0] + az_first[0])
    plan.task(
        "tok.all",
        3,
        0.02,
        waits=[f"twin{d}" for d in range(-(ny // 2) + 1, ny // 2 + 1)],
        after=[t for t in tok_ends.values() if t] + ["tok.own"],
    )

    k0 = 0.7978845608028654
    k1 = k0 * 0.044715

    lane = lax.broadcasted_iota(jnp.int32, (SUB, LANES), 1)

    def shifted(value, by):
        turned = pltpu.roll(value, by % rows, 1)
        if by > 0:
            edge = jnp.where(lane < by, 0.0, turned[:, :LANES])
            return jnp.concatenate([edge, turned[:, LANES:]], axis=1)
        edge = jnp.where(lane >= LANES + by, 0.0, turned[:, rows - LANES :])
        return jnp.concatenate([turned[:, : rows - LANES], edge], axis=1)

    def act_step(i):
        units = pl.ds(pl.multiple_of(i * SUB, SUB), SUB)
        g = gate[units, :].astype(F32)
        one, two = shifted(g, 1), shifted(g, 2)
        w0, w1, w2 = coef[units, 0:1], coef[units, 1:2], coef[units, 2:3]
        conv = coef[units, 3:4] + w0 * two + w1 * one + w2 * g
        square = conv * conv
        t = jnp.tanh(conv * (k0 + k1 * square))
        cdf = 0.5 + 0.5 * t
        slope = cdf + conv * (0.5 - 0.5 * (t * t)) * (k0 + (3.0 * k1) * square)
        hg = hidden[units, :].astype(F32)
        cg = slope * (hg * value[units, :].astype(F32))
        gg = w2 * cg + w1 * shifted(cg, -1) + w0 * shifted(cg, -2)
        for k, term in enumerate((cg * two, cg * one, cg * g, cg)):
            total = term[:, :LANES]
            for j in range(1, rows // LANES):
                total = total + term[:, j * LANES : (j + 1) * LANES]
            terms[k, units, :] = total
        at = jnp.where(i * SUB < whole, i * SUB, i * SUB + width)
        gt[pl.ds(pl.multiple_of(at, SUB), SUB), :] = gg.astype(BF16)
        at = i * SUB + whole
        gt[pl.ds(pl.multiple_of(at, SUB), SUB), :] = (hg * (conv * cdf)).astype(BF16)

    n_act = 11
    per_act = width // SUB // n_act

    def act(k):
        if k == 0:
            for name in ("gate", "value", "hidden", "cw", "cb"):
                loads[name].wait()
            taps[0:3, :width] = cw[...]
            taps[3, :width] = cb[...]
            coef[...] = taps[...].T

        def step(i, carry):
            act_step(k * per_act + i)
            return carry

        lax.fori_loop(0, per_act, step, 0)

    for k in range(n_act):
        plan.task(f"act{k}", 5, 1.2, functools.partial(act, k), after=[f"act{k - 1}"] if k else [])
    acted = f"act{n_act - 1}"

    pad = taps.shape[1]

    def conv_start():
        sums = jnp.concatenate([terms[k].T.sum(axis=0, keepdims=True) for k in range(4)], axis=0)
        cx[x] = jnp.concatenate([sums[:, : pad // 2], sums[:, pad // 2 :]], axis=0)

    def slots_ring(name, axis, slots):
        pair = slots.at[pl.ds(0, 2)]
        first, ends = gather(
            name, axis, lambda i: slots.at[i], lambda i, h: None if h else slots.at[i], pair, name, 4
        )
        return first, [t for t in ends.values() if t]

    cx_first, cx_names = slots_ring("cx", "x", cx)
    cz_first, cz_names = slots_ring("cz", "z", cz)
    ct_first, ct_names = slots_ring("ct", "x", ct)
    tiles = pad // 2 // LANES

    def total_of(slots, n):
        total = slots[0]
        for i in range(1, n):
            total = total + slots[i]
        return total

    def conv_middle():
        total = total_of(cx, nx)
        for j in range(tiles):
            csum[j] = total[:, j * LANES : (j + 1) * LANES]
        cz[z] = csum[jnp.minimum(x, tiles - 1)]

    def conv_late():
        ct[x] = total_of(cz, nz)

    def conv_end():
        total = jnp.concatenate([ct[j] for j in range(tiles)], axis=1) * scale
        total = jnp.concatenate([total[:4], total[4:]], axis=1)[:, :width]
        cwg_out[...] = total[:3]
        cbg_out[...] = total[3]

    plan.task("conv.start", 6, 0.2, conv_start, after=[acted], sends=cx_first)
    plan.task("conv.middle", 6, 0.1, conv_middle, after=cx_names + ["conv.start"], sends=cz_first)
    plan.task("conv.late", 6, 0.1, conv_late, after=cz_names + ["conv.middle"], sends=ct_first)
    plan.task("conv.end", 9, 0.1, conv_end, after=ct_names + ["conv.late"])

    grad_order = [nz // 2] + [s * h for h in range(nz // 2 - 1, 0, -1) for s in (1, -1)] + [0]

    def grad(d):
        to_z = (z + d + nz) % nz
        left = tok[:, pl.ds(pl.multiple_of(to_z * group, group), group)]
        over_rows = (((0,), (1,)), ((), ()))
        for right, out in ((gt.at[:ahead], pa), (gt.at[ahead:], pb)):
            part = lax.dot_general(left, right[...], over_rows, preferred_element_type=F32)
            out[pl.ds(to_z * nx, nx)] = part.astype(BF16).reshape(nx, shard, part.shape[1])

    for d in grad_order:
        plan.task(f"grad{d}", 7, 1.2, functools.partial(grad, d), after=["tok.all", acted])

    def ax_last(total):
        gg_out[:, :ahead] = total * scale

    def az_last(r, total):
        pa[z * nx + (x + r + nx) % nx] = total.astype(BF16)

    scatter(
        "pax",
        "x",
        lambda i: pa.at[z * nx + i],
        lambda i, h: pa.at[z * nx + i, pl.ds(h * shard // 2, shard // 2)],
        ax_up,
        ax_dn,
        lambda ref, j, h: ref.at[j, pl.ds(h * shard // 2, shard // 2)],
        pa.at[pl.ds(0, 2)],
        "pa",
        3,
        0.1,
        lambda d: [f"paz{d}.end"],
        ax_last,
    )
    for i, r in enumerate([nx // 2] + [s * h for h in range(nx // 2 - 1, 0, -1) for s in (1, -1)] + [0]):
        col = (x + r + nx) % nx
        scatter(
            f"paz{r}",
            "z",
            lambda i, col=col: pa.at[i * nx + col],
            lambda i, h, col=col: pa.at[i * nx + col, pl.ds(h * shard // 2, shard // 2)],
            az_up.at[i],
            az_dn.at[i],
            lambda ref, j, h: ref.at[j, pl.ds(h * shard // 2, shard // 2)],
            pa.at[pl.ds(0, 2)],
            "pa",
            2,
            0.1,
            lambda d: [f"grad{d}"],
            functools.partial(az_last, r),
        )

    def bz_last(total):
        total = total * scale
        start = whole - ahead
        gg_out[:, ahead:whole] = total[:, :start]
        vg_out[...] = total[:, start : start + width]
        gg_out[:, whole:] = total[:, start + width :]

    def bx_last(d, total):
        pb[((z + d + nz) % nz) * nx + x] = total.astype(BF16)

    for i, d in enumerate(grad_order):
        scatter(
            f"pbx{d}",
            "x",
            lambda i, d=d: pb.at[((z + d + nz) % nz) * nx + i],
            lambda i, h, d=d: pb.at[((z + d + nz) % nz) * nx + i, pl.ds(h * shard // 2, shard // 2)],
            bx_up.at[i],
            bx_dn.at[i],
            lambda ref, j, h: ref.at[j, pl.ds(h * shard // 2, shard // 2)],
            pb.at[pl.ds(0, 2)],
            "pb",
            2,
            0.1,
            lambda e, d=d: [f"grad{d}"],
            functools.partial(bx_last, d),
        )
    scatter(
        "pbz",
        "z",
        lambda i: pb.at[i * nx + x],
        lambda i, h: pb.at[i * nx + x, pl.ds(h * shard // 2, shard // 2)],
        bz_up,
        bz_dn,
        lambda ref, j, h: ref.at[j, pl.ds(h * shard // 2, shard // 2)],
        pb.at[pl.ds(0, 2)],
        "pb",
        2,
        0.1,
        lambda d: [f"pbx{d}.end"],
        bz_last,
    )


    def ig(d):
        at = (z + d + nz) % nz
        left_w = wa[pl.ds(at * nx, nx)].reshape(group, whole)
        right_w = wb[pl.ds(at * nx, nx)].reshape(group, 2 * width - whole)
        part = jnp.dot(left_w, gt[:whole], preferred_element_type=F32)
        part = part + jnp.dot(right_w, gt[whole:], preferred_element_type=F32)
        part = part.astype(BF16)
        for k in range(ny * NC):
            igp[at, k % NC, k // NC] = part[:, k * mine : (k + 1) * mine]

    for d in offsets_z:
        at = (z + d + nz) % nz
        m = f"igt{d}"
        source, target = igp.at[at, 1 - c], twin_in.at[at]
        plan.arrival(m, source)
        plan.message(m, "twin", source, target, twin, m, "ig")
        ends = [a[d] for a in az_ends.values()] + [bz_ends[d], *bx_ends[d].values()]
        ends = [t for t in ends if t]
        plan.task(f"ig{d}", 8, 1.1, functools.partial(ig, d), after=[acted] + ends, sends=[m])

        def merge(at=at):
            igp[at, c] = (igp[at, c].astype(F32) + twin_in[at].astype(F32)).astype(BF16)

        plan.task(f"igm{d}", 3, 0.2, merge, waits=[m], after=[f"ig{d}"])

        def ig_last(total, at=at):
            ig_out[:, pl.ds(pl.multiple_of(at * group, group), group)] = total.T.astype(BF16)

        scatter(
            f"igy{d}",
            "y",
            lambda i, at=at: igp.at[at, c, i],
            lambda i, h, at=at: igp.at[at, c, i, pl.ds(h * (group // 2), group // 2)],
            y_up.at[at],
            y_dn.at[at],
            lambda ref, j, h: ref.at[j, pl.ds(h * (group // 2), group // 2)],
            igp.at[0, 0, pl.ds(0, 2)],
            "ig",
            3,
            0.05,
            lambda e, d=d: [f"igm{d}"],
            ig_last,
        )

    left_from = {
        "wa": wa.at[pl.ds(0, nz * nx - 1)],
        "wb": wb.at[pl.ds(0, nz * nx - 1)],
        "tok": tok.at[pl.ds(0, (2 * ny - 1) * mine)],
        "pa": pa.at[pl.ds(0, nz * nx - 1)],
        "pb": pb.at[pl.ds(0, nz * nx - 1)],
        "ig": igp.at[pl.ds(0, nz * (2 * ny - 1) // (NC * ny))],
        "cx": cx.at[pl.ds(0, nx - 1)],
        "cz": cz.at[pl.ds(0, nz - 1)],
        "ct": ct.at[pl.ds(0, nx - 1)],
    }
    send_at = {name: send_sem.at[i] for i, name in enumerate(left_from)}
    recv_at = {name: recv_sem.at[i] for i, name in enumerate(plan.arrivals)}
    assert len(recv_at) == recv_sem.shape[0] and len(send_at) == send_sem.shape[0]
    for name, whole_ref in left_from.items():
        sizes = [nbytes_of(v[1]) for v in plan.messages.values() if v[5] == name]
        assert sum(sizes) == nbytes_of(whole_ref), name

    def remote(source, target, device, sent, arrival):
        return pltpu.make_async_remote_copy(
            src_ref=source,
            dst_ref=target,
            send_sem=send_at[sent],
            recv_sem=recv_at[arrival],
            device_id=device,
            device_id_type=MESH,
        )

    for name, (whole_ref, names) in plan.arrivals.items():
        assert sum(nbytes_of(plan.messages[m][2]) for m in names) == nbytes_of(whole_ref), name

    def start(m):
        link, source, target, device, arrival, sent = plan.messages[m]
        remote(source, target, device, sent, arrival).start()

    for name in plan.order():
        rank, cost, body, waits, after, sends = plan.tasks[name]
        for w in waits:
            ref, names = plan.arrivals[w]
            remote(ref, ref, twin, plan.messages[names[0]][5], w).wait_recv()
        if isinstance(body, tuple):
            body[0](start)
            continue
        if body is not None:
            body()
        for m in sends:
            start(m)
    for name, ref in left_from.items():
        remote(ref, ref, twin, name, next(iter(recv_at))).wait_send()


def put_out(*refs):
    copies = [pltpu.make_async_copy(refs[i], refs[5 + i], refs[10].at[i]) for i in range(5)]
    for copy in copies:
        copy.start()
    for copy in copies:
        copy.wait()


def on_device(dims, *args):
    tokens, gate_pre, value_pre, up_gate_w, up_value_w, conv_weight, conv_bias, hidden_grad = args
    nz, nx, ny = dims
    rows, width = gate_pre.shape
    mine, model = tokens.shape
    shard = up_gate_w.shape[0]
    whole = width // LANES * LANES
    ca, cb = whole, 2 * width - whole
    pa, pb = whole - LANES, 2 * width - whole + LANES
    pad = whole + LANES
    group = nx * shard
    n_arrivals = (4 + 2 * nz) * (nx // 2) + (3 + 2 * nx) * (nz // 2) + (nz + 1) * (ny // 2) + ny + nz
    outs = (
        ((mine, model), BF16),
        ((shard, width), F32),
        ((shard, width), F32),
        ((3, width), F32),
        ((width,), F32),
    )
    results = pl.pallas_call(
        functools.partial(kernel, dims),
        out_shape=[pltpu.VMEM(*out) for out in outs],
        in_specs=[pl.BlockSpec(memory_space=pltpu.HBM)] * 8,
        out_specs=[pl.BlockSpec(memory_space=pltpu.VMEM)] * 5,
        scratch_shapes=[
            pltpu.VMEM((width, rows), BF16),
            pltpu.VMEM((width, rows), BF16),
            pltpu.VMEM((width, rows), BF16),
            pltpu.VMEM((shard, width), BF16),
            pltpu.VMEM((shard, width), BF16),
            pltpu.VMEM((3, width), F32),
            pltpu.VMEM((width,), F32),
            pltpu.VMEM((mine * ny * NC, model), BF16),
            pltpu.VMEM((nz * nx, shard, ca), BF16),
            pltpu.VMEM((nz * nx, shard, cb), BF16),
            pltpu.VMEM((2 * width, rows), BF16),
            pltpu.VMEM((nz * nx, shard, pa), BF16),
            pltpu.VMEM((nz * nx, shard, pb), BF16),
            pltpu.VMEM((nx, nz // 2, shard, pa), BF16),
            pltpu.VMEM((nx, nz // 2, shard, pa), BF16),
            pltpu.VMEM((nx // 2, shard, pa), BF16),
            pltpu.VMEM((nx // 2, shard, pa), BF16),
            pltpu.VMEM((nz, nx // 2, shard, pb), BF16),
            pltpu.VMEM((nz, nx // 2, shard, pb), BF16),
            pltpu.VMEM((nz // 2, shard, pb), BF16),
            pltpu.VMEM((nz // 2, shard, pb), BF16),
            pltpu.VMEM((nz, NC, ny, group, mine), BF16),
            pltpu.VMEM((nz, ny, group, mine), BF16),
            pltpu.VMEM((nz, ny // 2, group, mine), BF16),
            pltpu.VMEM((nz, ny // 2, group, mine), BF16),
            pltpu.VMEM((8, pad), F32),
            pltpu.VMEM((pad, 8), F32),
            pltpu.VMEM((4, pad, LANES), F32),
            pltpu.VMEM((nx, 8, pad // 2), F32),
            pltpu.VMEM((nz, 8, LANES), F32),
            pltpu.VMEM((nx, 8, LANES), F32),
            pltpu.VMEM((pad // 2 // LANES, 8, LANES), F32),
            pltpu.SemaphoreType.DMA((8,)),
            pltpu.SemaphoreType.DMA((9,)),
            pltpu.SemaphoreType.DMA((n_arrivals,)),
        ],
        compiler_params=pltpu.CompilerParams(
            collective_id=0, has_side_effects=True, vmem_limit_bytes=56_000_000
        ),
    )(
        *(
            pltpu.with_memory_space_constraint(a, pltpu.HBM)
            for a in (
                tokens,
                gate_pre.T,
                value_pre.T,
                up_gate_w,
                up_value_w,
                conv_weight,
                conv_bias,
                hidden_grad.T,
            )
        )
    )
    return pl.pallas_call(
        put_out,
        out_shape=[jax.ShapeDtypeStruct(*out) for out in outs],
        in_specs=[pl.BlockSpec(memory_space=pltpu.VMEM)] * 5,
        out_specs=[pl.BlockSpec(memory_space=pltpu.HBM)] * 5,
        scratch_shapes=[pltpu.SemaphoreType.DMA((5,))],
    )(*(pltpu.with_memory_space_constraint(r, pltpu.VMEM) for r in results))


def solution(mesh):
    sizes = (mesh.shape["fs"], mesh.shape["tp"])
    dims = {(32, 8): (8, 4, 4)}[sizes]
    in_specs = (
        P(("fs", "tp"), None),
        P("fs", "tp"),
        P("fs", "tp"),
        P("fs", "tp"),
        P("fs", "tp"),
        P(None, "tp"),
        P("tp"),
        P("fs", "tp"),
    )
    out_specs = (P(("fs", "tp"), None), P("fs", "tp"), P("fs", "tp"), P(None, "tp"), P("tp"))
    return jax.shard_map(
        functools.partial(on_device, dims),
        mesh=mesh,
        in_specs=in_specs,
        out_specs=out_specs,
        check_vma=False,
    )
```
